32 devices in a mesh: grp: 2 (over y), sp: 4 (over z), tp: 4 (over x, core).
Axes of the slice: x: 2, y: 2, z: 4, core: 2. Of those that a mesh axis runs over, the one named last changes fastest.
Arguments:
- stream: bfloat16 [6144, 4096], P(('grp', 'sp'), 'tp'), parts along dimension 0, may hold values from -400 to 400
- in_weight: bfloat16 [2, 1024, 4096], P(None, 'sp', 'tp'), may hold values from -0.09375 to 0.09375
- out_weight: bfloat16 [2, 1024, 4096], P(None, 'sp', 'tp'), may hold values from -0.1875 to 0.1875
- group_mix: bfloat16 [2, 4, 256, 256], replicated, may hold values from -0.375 to 0.375
- pool_gain: float32 [2, 1024], replicated, may hold values from 0.1 to 1.9
- norm_gain: float32 [2, 4096], P(None, 'tp'), may hold values from 0.1 to 1.9
- norm_shift: float32 [2, 4096], P(None, 'tp'), may hold values from -3 to 3
Outputs:
- refined: bfloat16 [6144, 4096], P(('grp', 'sp'), 'tp'), parts along dimension 0
The draws below stay inside these ranges and needn't reach their ends.
There are 2 independent parts, one for each index of `grp`. The reference program is written for one: setup_inputs(seed, part) draws one part's arguments, and reference() takes and returns one part's arrays. A program takes and returns all parts, laid end to end along the dimension named above; an argument that names none is the same for every part. Nothing has to cross between parts.
All inputs are finite; a program needn't handle non-finite values.
Results may differ from the reference program's by a relative error of at most 0.015.
Values may be sent and summed in bfloat16 or wider, within the bound.
A program may use at most 64 MiB of HBM per device.

```python
import jax
import jax.numpy as jnp
from jax import lax

D = 4096
POOL = 1024
GROUPS = 4
GROUP_WIDTH = 256
LAYERS = 2
TOKENS = 3072
N_TP = 4


def draw_stream(key, part):
    base = jax.random.fold_in(key, 17)
    first_key, second_key = jax.random.split(base, 2)
    column = jnp.arange(D, dtype=jnp.float32) / D
    row_scale = 10.0 ** jax.random.uniform(second_key, (TOKENS, 1), jnp.float32)
    entries = jnp.clip(jax.random.normal(first_key, (TOKENS, D), jnp.float32), -4.0, 4.0)
    column_scale = 10.0 ** column
    return (entries * column_scale[None, :] * row_scale).astype(jnp.bfloat16)


def steps_of(rng, extent, cuts, smallest, high):
    factor_of, own = 1.0, jax.random.fold_in(rng, 6)
    for axis_at, shards_of in cuts:
        steps = jnp.exp(jax.random.uniform(jax.random.fold_in(own, axis_at), (shards_of,), jnp.float32, smallest / len(cuts), high / len(cuts)))
        factor_of = factor_of * jnp.repeat(steps, extent[axis_at] // shards_of).reshape([-1 if axis == axis_at else 1 for axis in range(len(extent))])
    return factor_of


def centred(stream_key, dims, scale, bound, cuts=(), kind=jnp.bfloat16):
    array = jax.random.normal(stream_key, dims, jnp.float32) * scale
    if len(cuts) > 0:
        array = steps_of(stream_key, dims, cuts, -0.22, 0.18) * array
    return jnp.clip(array, min=-bound, max=bound).astype(kind)


def setup_inputs(seed: int = 0, part: int = 0) -> dict:
    seeds = jax.random.split(jax.random.key(seed), 8)
    own_keys = jax.random.split(jax.random.fold_in(seeds[7], part), 8)
    return {
        "stream": draw_stream(jax.random.fold_in(jax.random.fold_in(seeds[7], part), 71), part),
        "in_weight": centred(seeds[1], (LAYERS, POOL, D), D ** -0.5, 0.09375, ((1, 4), (2, 4))),
        "out_weight": centred(seeds[2], (LAYERS, POOL, D), POOL ** -0.5, 0.1875, ((1, 4), (2, 4))),
        "group_mix": centred(seeds[3], (LAYERS, GROUPS, GROUP_WIDTH, GROUP_WIDTH), GROUP_WIDTH ** -0.5, 0.375),
        "pool_gain": jnp.clip(1.0 + 0.18 * jax.random.normal(seeds[4], (LAYERS, POOL), jnp.float32), 0.1, 1.9),
        "norm_gain": jnp.clip(1.0 + 0.18 * jax.random.normal(seeds[5], (LAYERS, D), jnp.float32), 0.1, 1.9),
        "norm_shift": centred(seeds[6], (LAYERS, D), 0.5, 3.0, ((1, 4),), jnp.float32),
    }


epsilon = 1e-05

def reference(stream, in_weight, out_weight, group_mix, pool_gain, norm_gain, norm_shift):
    tokens_total = stream.shape[0]
    channel_block = D // N_TP
    alpha = (2.0 * LAYERS) ** 0.25
    current = stream
    for layer_index in range(LAYERS):
        hidden_sum = jnp.zeros((tokens_total, POOL), jnp.float32)
        for part_index in range(N_TP):
            lower = part_index * channel_block
            upper = lower + channel_block
            term = jnp.dot(current[:, lower:upper], in_weight[layer_index][:, lower:upper].T, preferred_element_type=jnp.float32)
            rounded = lax.optimization_barrier(term.astype(jnp.bfloat16))
            hidden_sum = hidden_sum + rounded.astype(jnp.float32)
        hidden = hidden_sum.astype(jnp.bfloat16)
        positions = jnp.arange(1, tokens_total + 1, dtype=jnp.float32)[:, None]
        pooled_pieces = []
        for group_index in range(GROUPS):
            width = 2 ** (group_index + 1)
            group_cols = hidden[:, group_index * GROUP_WIDTH:(group_index + 1) * GROUP_WIDTH].astype(jnp.float32)
            padded = jnp.pad(group_cols, ((width - 1, 0), (0, 0)))
            window_sum = jnp.zeros_like(group_cols)
            for offset in range(width):
                window_sum = window_sum + padded[offset:offset + tokens_total]
            counts = jnp.minimum(positions, float(width))
            pooled_pieces.append(window_sum / counts - group_cols)
        pooled = jnp.concatenate(pooled_pieces, axis=1).astype(jnp.bfloat16)
        mixed_pieces = []
        for group_index in range(GROUPS):
            group_rows = pooled[:, group_index * GROUP_WIDTH:(group_index + 1) * GROUP_WIDTH]
            mixed_pieces.append(jnp.dot(group_rows, group_mix[layer_index, group_index], preferred_element_type=jnp.float32))
        scaled = (jnp.concatenate(mixed_pieces, axis=1) * pool_gain[layer_index][None, :]).astype(jnp.bfloat16)
        branch = jnp.dot(scaled, out_weight[layer_index], preferred_element_type=jnp.float32)
        summed = alpha * current.astype(jnp.float32) + branch
        row_mean = lax.optimization_barrier(jnp.sum(summed, axis=1)) / D
        row_var = lax.optimization_barrier(jnp.sum(summed * summed, axis=1)) / D - row_mean * row_mean
        normed = (summed - row_mean[:, None]) * lax.rsqrt(row_var + epsilon)[:, None]
        current = (normed * norm_gain[layer_index][None, :] + norm_shift[layer_index][None, :]).astype(jnp.bfloat16)
    return current
```

```python
import functools

import jax
import jax.numpy as jnp
from jax import lax
from jax.experimental import pallas as pl
from jax.experimental.pallas import tpu as pltpu
from jax.sharding import PartitionSpec as P

MESH = pl.DeviceIdType.MESH
EPSILON = 1e-05
F32 = jnp.float32
BF16 = jnp.bfloat16
REACH = 16
PIECES = 4
STEPS = (
    ("project", 0), ("chip_sum", 0), ("project", 1), ("chip_sum", 1), ("project", 2), ("chip_sum",
    2), ("project", 3), ("chip_sum", 3), ("finish_hidden", 0), ("pool", 0), ("finish_hidden", 1),
    ("pool", 1), ("expand", 0), ("finish_hidden", 2), ("pool", 2), ("expand", 1), ("finish_hidden",
    3), ("pool", 3), ("expand", 2), ("expand", 3), ("norm", 0), ("norm", 1),
)
EDGE_TICKS = (4, 6, 7, 9, 11, 13, 15, 17, 17, 17, 17, 17, 18, 19, 19, 19, 22, 22, 23, 27, 29, 30, 30, 32, 32,
    33, 35, 37, 39, 41, 41, 41, 41, 41, 42, 43, 43, 44, 47, 47, 47, 48, 48, 48)
INNER_TICKS = (8, 10, 11, 12, 12, 16, 18, 20, 20, 20, 22, 22, 22, 25, 25, 26, 30, 30, 31, 33, 35, 35, 35, 37,
    37, 38, 38, 40, 40, 40, 41, 41, 45, 45, 46, 48, 48, 48, 48, 48, 48, 48, 48, 48)
INNER_ORDER = (1, 2, 1, 2, 1, 2, 1, 2, 3, 3, 3, 3, 1, 2, 1, 2, 1, 2, 1, 2, 3, 3, 3, 3, 1, 1, 1, 2, 1, 2, 2, 3,
    2, 3, 3, 3, 1, 1, 1, 1, 2, 2, 2, 3, 2, 3, 3, 3)
NT = (((1,), (1,)), ((), ()))


def arrival_orders(n):
    orders = []
    for z in range(n):
        first = 1 if z < n / 2 else -1
        order = [z]
        for d in range(1, n):
            order += [b for b in (z + first * d, z - first * d) if 0 <= b < n]
        orders.append(order)
    return orders


def stream_plan(n, layers):
    ms = 2 * layers
    edge = [(m, s, q) for m in range(ms) for s in range(1, n) for q in range(PIECES)]
    seen = [0] * n
    inner = []
    for s in INNER_ORDER:
        inner.append((seen[s] // PIECES, s, seen[s] % PIECES))
        seen[s] += 1
    return edge, inner


def kernel(cfg, *refs):
    n, tp_n, layers, groups, width, streamed = cfg
    (stream, w_in, w_out, mix_in, gain_in, norm_gain_in, norm_shift_in, out,
     mix, gain, norm_gain, norm_shift, wg, cur, acc, psend, precv, pown, xsend, xrecv, hbuf, sc, tsend, trecv, esend, erecv,
     loc_sem, own_send, rest_send, f_send, z_recv, y_send, y_recv,
     p_send_s, p_recv_s, x_send_s, x_recv_s, halo_s,
     c_send_s, c_recv_s, t_send_s, t_recv_s, e_send_s, e_recv_s) = refs
    tokens, chans = stream.shape
    half = tokens // 2
    halo = layers * REACH
    ahead = halo - REACH
    reach_rows = half + halo
    part_rows = half + ahead
    d_model = chans * tp_n
    alpha = (2.0 * layers) ** 0.25
    nx = tp_n // 2
    y, z, t = lax.axis_index("grp"), lax.axis_index("sp"), lax.axis_index("tp")
    core, x = lax.rem(t, 2), t // 2
    sib = t + 1 - 2 * core
    orders = arrival_orders(n)
    mine, other = core * half, (1 - core) * half
    mine = pl.multiple_of(mine, REACH)
    other = pl.multiple_of(other, REACH)

    def order(s):
        if not streamed:
            return jnp.int32(s)
        b = jnp.int32(0)
        for k in range(n):
            b = jnp.where(z == k, orders[k][s], b)
        return b

    def remote(src, dst, ssem, rsem, device):
        return pltpu.make_async_remote_copy(
            src_ref=src, dst_ref=dst, send_sem=ssem, recv_sem=rsem,
            device_id=device, device_id_type=MESH)

    barrier = pltpu.get_barrier_semaphore()

    def greet(device):
        pl.semaphore_signal(barrier, inc=1, device_id=device, device_id_type=MESH)

    for k in range(1, tp_n):
        greet((y, z, lax.rem(t + k, tp_n)))
    count = jnp.int32(tp_n - 1)
    if streamed:
        greet((1 - y, z, t))
        count = count + 1

    @pl.when(z > 0)
    def _():
        greet((y, z - 1, t))

    @pl.when(z < n - 1)
    def _():
        greet((y, z + 1, t))

    count = count + jnp.where(z > 0, 1, 0) + jnp.where(z < n - 1, 1, 0)
    rows = w_in.shape[1]
    copies = [pltpu.make_async_copy(stream, cur.at[pl.ds(halo, tokens)], loc_sem.at[0])]
    for m in range(2 * layers):
        src = (w_in, w_out)[m % 2].at[m // 2]
        if streamed:
            dst = wg.at[m, pl.ds(pl.multiple_of(z * rows, rows), rows)]
        else:
            dst = wg.at[m]
        copies.append(pltpu.make_async_copy(src, dst, loc_sem.at[1 + m]))
    for at, pair in enumerate(((mix_in, mix), (gain_in, gain), (norm_gain_in, norm_gain), (norm_shift_in, norm_shift))):
        copies.append(pltpu.make_async_copy(*pair, loc_sem.at[1 + 2 * layers + at]))
    for copy in copies:
        copy.start()

    pl.semaphore_wait(barrier, count)

    part = rows // 2
    cut = part // PIECES

    def span(base, q):
        return pl.ds(pl.multiple_of(base + q * cut, cut), cut)

    edge = (z == 0) | (z == n - 1)

    def own_copy(m, side, q):
        src = (w_in, w_out)[m % 2].at[m // 2, span(y * part, q)]
        dst = wg.at[m, span(z * rows + y * part, q)]
        return remote(src, dst, own_send.at[m, side, q], z_recv.at[m, z, q], (y, z + 2 * side - 1, t))

    def rest_copy(m, q):
        src = (w_in, w_out)[m % 2].at[m // 2, span((1 - y) * part, q)]
        dst = wg.at[m, span(z * rows + (1 - y) * part, q)]
        return remote(src, dst, rest_send.at[m, q], y_recv.at[m, z, q],
                      (y, jnp.where(z == 0, 1, n - 2), t))

    def own_start(m, k, side):
        if not 0 <= k + 2 * side - 1 < n:
            return

        @pl.when(z == k)
        def _():
            for q in range(PIECES):
                own_copy(m, side, q).start()
            if m == 0 and side:
                halo_copy().start()
            if k in (0, n - 1):
                for q in range(PIECES):
                    rest_copy(m, q).start()

    def onward(m, b, q):
        zt = jnp.where(b < z, z + 1, z - 1)
        ref = wg.at[m, span(b * rows + y * part, q)]
        return (zt >= 0) & (zt < n), remote(
            ref, ref, f_send.at[m, b, q], z_recv.at[m, b, q], (y, zt, t))

    def whole(b):
        return ((z == 1) & (b == 0)) | ((z == n - 2) & (b == n - 1))

    def across(m, b, from_y, q):
        ref = wg.at[m, span(b * rows + from_y * part, q)]
        return remote(ref, ref, y_send.at[m, b, q], y_recv.at[m, b, q], (1 - y, z, t))

    def by_place(values):
        picked = jnp.int32(values[0])
        for k in range(1, n):
            if values[k] != values[0]:
                picked = jnp.where(z == k, values[k], picked)
        return picked

    edge_events, inner_events = stream_plan(n, layers)
    state = [0, 0]

    def take(e_event, i_event):
        places = [k for k in range(n) if (e_event if k in (0, n - 1) else i_event)]

        def go():
            vals = [(e_event if k in (0, n - 1) else i_event) or e_event or i_event for k in range(n)]
            m = by_place([v[0] for v in vals])
            b = by_place([orders[k][v[1]] for k, v in enumerate(vals)])
            q = by_place([v[2] for v in vals])
            there, copy = onward(m, b, q)
            copy.wait_recv()
            pl.when(there)(copy.start)
            pl.when(jnp.logical_not(whole(b)))(across(m, b, y, q).start)

        if len(places) == n:
            go()
        else:
            pl.when(edge if e_event else jnp.logical_not(edge))(go)
        for k in places:
            m, s, q = e_event if k in (0, n - 1) else i_event
            if q != PIECES - 1 or m + 1 >= 2 * layers:
                continue
            if k in (0, n - 1):
                if s == 1:
                    own_start(m + 1, k, 1 if k == 0 else 0)
            elif s == n - 1:
                own_start(m + 1, k, 0 if k < n / 2 else 1)
            elif s == 2:
                own_start(m + 1, k, 1 if k < n / 2 else 0)

    def tick(e_goal, i_goal):
        if not streamed:
            return
        while state[0] < e_goal or state[1] < i_goal:
            e_event = i_event = None
            if state[0] < e_goal:
                e_event = edge_events[state[0]]
                state[0] += 1
            if state[1] < i_goal:
                i_event = inner_events[state[1]]
                state[1] += 1
            take(e_event, i_event)

    def ready(m, s):
        if s == 0:
            copies[1 + m].wait()
        elif streamed:
            for q in range(PIECES):
                across(m, order(s), 1 - y, q).wait_recv()

    def weight(m, s):
        return wg[m, pl.ds(pl.multiple_of(order(s) * width, width), width), :]

    def p_copy(l, s):
        return remote(psend.at[l, s], precv.at[l, s], p_send_s.at[l, s], p_recv_s.at[l, s], (y, z, sib))

    def x_copies(l, s):
        return [remote(xsend.at[l, s], xrecv.at[k - 1, l, s], x_send_s.at[k - 1, l, s],
                       x_recv_s.at[k - 1, l, s], (y, z, lax.rem(x + k, nx) * 2 + core))
                for k in range(1, nx)]

    def halo_copy():
        return remote(stream.at[pl.ds(tokens - halo, halo)], cur.at[pl.ds(0, halo)],
                      halo_s.at[0], halo_s.at[1], (y, jnp.minimum(z + 1, n - 1), t))

    def c_copy(l, s, side):
        ref = sc.at[l, s, side]
        return remote(ref, ref, c_send_s.at[l, s], c_recv_s.at[l, s], (y, z, sib))

    def t_copies(l, i):
        return [remote(tsend.at[l, i], trecv.at[k - 1, l, i], t_send_s.at[k - 1, l, i],
                       t_recv_s.at[k - 1, l, i], (y, z, lax.rem(t + k, tp_n)))
                for k in range(1, tp_n)]

    def e_copies(l):
        return [remote(esend.at[l], erecv.at[k - 1, l], e_send_s.at[k - 1, l],
                       e_recv_s.at[k - 1, l], (y, z, lax.rem(t + k, tp_n)))
                for k in range(1, tp_n)]

    def project(l, s):
        w = weight(2 * l, s)
        psend[l, s] = lax.dot_general(
            cur[pl.ds(other, reach_rows), :], w, NT, preferred_element_type=F32).astype(BF16)
        p_copy(l, s).start()
        pown[s] = lax.dot_general(cur[pl.ds(mine, reach_rows), :], w, NT, preferred_element_type=F32)

    def chip_sum(l, s):
        p_copy(l, s).wait_recv()
        total = pown[s] + precv[l, s].astype(F32)
        pown[s] = total
        xsend[l, s] = total.astype(BF16)
        for copy in x_copies(l, s):
            copy.start()

    def finish_hidden(l, s):
        total = pown[s]
        for k, copy in enumerate(x_copies(l, s)):
            copy.wait_recv()
            total = total + xrecv[k, l, s].astype(F32)
        hbuf[s] = total.astype(BF16).astype(F32)

        @pl.when((z == 0) & (core == 0))
        def _():
            hbuf[s, :halo, :] = jnp.zeros((halo, width), F32)

    def pool(l, s):
        b = order(s)
        ext = hbuf[s]
        run = ext + pltpu.roll(ext, 1, 0)
        for octave in range(1, groups):
            take = jnp.where(b >= octave, 1.0, 0.0).astype(F32)
            run = run + take * pltpu.roll(run, 2**octave, 0)
        reach = jnp.int32(2)
        for octave in range(1, groups):
            reach = jnp.where(b >= octave, 2 ** (octave + 1), reach)
        at = z * tokens + core * half - ahead + 1 + lax.broadcasted_iota(jnp.int32, (part_rows, width), 0)
        counts = jnp.clip(at, 1, reach).astype(F32)
        pooled = (run[REACH:, :] / counts - ext[REACH:, :]).astype(BF16)
        mixed = jnp.dot(pooled, mix[l, b], preferred_element_type=F32)
        sc[l, s, core] = (mixed * gain[l:l + 1, pl.ds(pl.multiple_of(b * width, width), width)]).astype(BF16)
        c_copy(l, s, core).start()

    def grow(l, s, add, rows_at, cur_at):
        if s == 0:
            acc[rows_at, :] = alpha * cur[cur_at, :].astype(F32) + add
        else:
            acc[rows_at, :] = acc[rows_at, :] + add

    def row_totals(v):
        lane = lax.broadcasted_iota(jnp.int32, (v.shape[0], 128), 1)
        row_sum = jnp.sum(v, axis=1, keepdims=True)
        row_squares = jnp.sum(v * v, axis=1, keepdims=True)
        return jnp.where(lane == 0, row_sum, jnp.where(lane == 1, row_squares, 0.0))

    def expand(l, s):
        c_copy(l, s, 1 - core).wait_recv()
        at_m = 2 * l + 1
        extra = l * REACH

        if extra < ahead:
            add = jnp.dot(sc[l, s, 0, extra:ahead, :], weight(at_m, s), preferred_element_type=F32)
            grow(l, s, add, slice(extra, ahead), slice(extra + REACH, halo))
            if s == groups - 1:
                esend[l, extra:, :] = row_totals(acc[extra:ahead, :])
                for copy in e_copies(l):
                    copy.start()

        def body(i, carry):
            add = jnp.dot(sc[l, s, i, ahead:, :], weight(at_m, s), preferred_element_type=F32)
            at = i * half
            if not isinstance(i, int):
                at = pl.multiple_of(at, REACH)
            grow(l, s, add, pl.ds(ahead + at, half), pl.ds(halo + at, half))
            return carry

        if s < groups - 1:
            lax.fori_loop(0, 2, body, 0)
            return
        for i in range(2):
            body(i, 0)
            both = row_totals(acc[ahead + i * half:ahead + (i + 1) * half, :])
            tsend[l, i] = both.T[:8, :]
            for copy in t_copies(l, i):
                copy.start()

    def norm(l, i):
        dst, base = (out, 0) if l == layers - 1 else (cur, halo)
        extra = l * REACH

        def apply(at, mean, inv, size):
            v = (acc[at:at + size, :] - mean) * inv
            to = at - ahead + base
            dst[to:to + size, :] = (v * norm_gain[l:l + 1, :] + norm_shift[l:l + 1, :]).astype(BF16)

        if extra < ahead and i == 0:
            stats = esend[l, extra:, :]
            for k, copy in enumerate(e_copies(l)):
                copy.wait_recv()
                stats = stats + erecv[k, l, extra:, :]
            stats = stats / d_model
            mean = stats[:, 0:1]
            inv = lax.rsqrt(stats[:, 1:2] - mean * mean + EPSILON)
            apply(extra, mean, inv, ahead - extra)
        stats = tsend[l, i]
        for k, copy in enumerate(t_copies(l, i)):
            copy.wait_recv()
            stats = stats + trecv[k, l, i]
        stats = stats / d_model
        mean = stats[0:1, :]
        var = stats[1:2, :] - mean * mean
        inv = lax.rsqrt(var + EPSILON)
        row = lax.broadcasted_iota(jnp.int32, (128, half), 0)
        cols = jnp.where(row == 0, mean, jnp.where(row == 1, inv, 0.0)).T
        apply(ahead + i * half, cols[:, 0:1], cols[:, 1:2], half)

    if streamed:
        for k in range(n):
            for side in (1, 0):
                own_start(0, k, side)
    else:
        pl.when(z < n - 1)(halo_copy().start)

    def before_first():
        @pl.when(z > 0)
        def _():
            halo_copy().wait_recv()

        @pl.when(z == 0)
        def _():
            cur[:halo, :] = jnp.zeros((halo, chans), BF16)

        copies[0].wait()
        for copy in copies[1 + 2 * layers:]:
            copy.wait()

    phases = {"project": project, "chip_sum": chip_sum, "finish_hidden": finish_hidden,
              "pool": pool, "expand": expand, "norm": norm}
    at = 0
    for l in range(layers):
        for name, s in STEPS:
            if at < len(EDGE_TICKS):
                tick(EDGE_TICKS[at], INNER_TICKS[at])
            if at == 0:
                before_first()
            if name == "project":
                ready(2 * l, s)
            elif name == "expand":
                ready(2 * l + 1, s)
            phases[name](l, s)
            at += 1

    if streamed:
        for m in range(2 * layers):
            for side in (1, 0):
                @pl.when((z < n - 1) if side else (z > 0))
                def _():
                    for q in range(PIECES):
                        own_copy(m, side, q).wait_send()

            @pl.when(edge)
            def _():
                for q in range(PIECES):
                    rest_copy(m, q).wait_send()

            for s in range(1, n):
                b = order(s)
                for q in range(PIECES):
                    there, copy = onward(m, b, q)
                    pl.when(there)(copy.wait_send)
                    pl.when(jnp.logical_not(whole(b)))(across(m, b, y, q).wait_send)
    for l in range(layers):
        for s in range(groups):
            p_copy(l, s).wait_send()
            for copy in x_copies(l, s):
                copy.wait_send()
            c_copy(l, s, core).wait_send()
        for i in range(2):
            for copy in t_copies(l, i):
                copy.wait_send()
        if l * REACH < ahead:
            for copy in e_copies(l):
                copy.wait_send()
    pl.when(z < n - 1)(halo_copy().wait_send)


def per_device(n, grp_n, tp_n, stream, in_weight, out_weight, group_mix, pool_gain, norm_gain, norm_shift):
    layers, groups, width = group_mix.shape[:3]
    tokens, chans = stream.shape
    pool = groups * width
    streamed = n == groups == 4 and grp_n == 2 and layers == 2
    if not streamed:
        in_weight = lax.all_gather(in_weight, "sp", axis=1, tiled=True)
        out_weight = lax.all_gather(out_weight, "sp", axis=1, tiled=True)
    nx = tp_n // 2
    half = tokens // 2
    halo = layers * REACH
    ahead = halo - REACH
    ms = 2 * layers
    dma = pltpu.SemaphoreType.DMA
    any_spec = pl.BlockSpec(memory_space=pl.ANY)
    vmem = pl.BlockSpec(memory_space=pltpu.VMEM)
    xs = max(nx - 1, 1)
    return pl.pallas_call(
        functools.partial(kernel, (n, tp_n, layers, groups, width, streamed)),
        out_shape=jax.ShapeDtypeStruct((tokens, chans), BF16),
        in_specs=[any_spec] * 7,
        out_specs=vmem,
        scratch_shapes=[
            pltpu.VMEM(group_mix.shape, BF16),
            pltpu.VMEM(pool_gain.shape, F32),
            pltpu.VMEM(norm_gain.shape, F32),
            pltpu.VMEM(norm_shift.shape, F32),
            pltpu.VMEM((ms, pool, chans), BF16),
            pltpu.VMEM((halo + tokens, chans), BF16),
            pltpu.VMEM((ahead + tokens, chans), F32),
            pltpu.VMEM((layers, groups, halo + half, width), BF16),
            pltpu.VMEM((layers, groups, halo + half, width), BF16),
            pltpu.VMEM((groups, halo + half, width), F32),
            pltpu.VMEM((layers, groups, halo + half, width), BF16),
            pltpu.VMEM((xs, layers, groups, halo + half, width), BF16),
            pltpu.VMEM((groups, halo + half, width), F32),
            pltpu.VMEM((layers, groups, 2, ahead + half, width), BF16),
            pltpu.VMEM((layers, 2, 8, half), F32),
            pltpu.VMEM((tp_n - 1, layers, 2, 8, half), F32),
            pltpu.VMEM((layers, ahead, 128), F32),
            pltpu.VMEM((tp_n - 1, layers, ahead, 128), F32),
            dma((5 + ms,)),
            dma((ms, 2, PIECES)), dma((ms, PIECES)), dma((ms, groups, PIECES)), dma((ms, groups, PIECES)),
            dma((ms, groups, PIECES)), dma((ms, groups, PIECES)),
            dma((layers, groups)), dma((layers, groups)),
            dma((xs, layers, groups)), dma((xs, layers, groups)),
            dma((2,)),
            dma((layers, groups)), dma((layers, groups)),
            dma((tp_n - 1, layers, 2)), dma((tp_n - 1, layers, 2)),
            dma((tp_n - 1, layers)), dma((tp_n - 1, layers)),
        ],
        compiler_params=pltpu.CompilerParams(
            collective_id=0, has_side_effects=True, vmem_limit_bytes=56 * 1024 * 1024),
    )(stream, in_weight, out_weight, group_mix,
      pool_gain, norm_gain, norm_shift)


def solution(mesh):
    in_specs = (
        P(("grp", "sp"), "tp"),
        P(None, "sp", "tp"),
        P(None, "sp", "tp"),
        P(),
        P(),
        P(None, "tp"),
        P(None, "tp"),
    )
    out_specs = P(("grp", "sp"), "tp")
    sizes = mesh.shape
    body = functools.partial(per_device, sizes["sp"], sizes["grp"], sizes["tp"])
    return jax.shard_map(
        body, mesh=mesh, in_specs=in_specs, out_specs=out_specs, check_vma=False
    )
```

```python
import functools

import jax
import jax.numpy as jnp
from jax import lax
from jax.experimental import pallas as pl
from jax.experimental.pallas import tpu as pltpu
from jax.sharding import PartitionSpec as P

MESH = pl.DeviceIdType.MESH
EPSILON = 1e-05
F32 = jnp.float32
BF16 = jnp.bfloat16
REACH = 16
PIECES = 4
STEPS = (
    ("project", 0), ("chip_sum", 0), ("project", 1), ("chip_sum", 1), ("project", 2), ("chip_sum",
    2), ("project", 3), ("chip_sum", 3), ("finish_hidden", 0), ("pool", 0), ("finish_hidden", 1),
    ("pool", 1), ("expand", 0), ("finish_hidden", 2), ("pool", 2), ("expand", 1), ("finish_hidden",
    3), ("pool", 3), ("expand", 2), ("expand", 3), ("norm", 0), ("norm", 1),
)
EDGE_TICKS = (4, 6, 7, 9, 11, 13, 15, 17, 17, 17, 17, 17, 18, 19, 19, 19, 22, 22, 23, 27, 29, 30, 30, 32, 32,
    33, 35, 37, 39, 41, 41, 41, 41, 41, 42, 43, 43, 44, 47, 47, 47, 48, 48, 48)
INNER_TICKS = (8, 10, 11, 12, 12, 16, 18, 20, 20, 20, 22, 22, 22, 25, 25, 26, 30, 30, 31, 33, 35, 35, 35, 37,
    37, 38, 38, 40, 40, 40, 41, 41, 45, 45, 46, 48, 48, 48, 48, 48, 48, 48, 48, 48)
INNER_ORDER = (1, 2, 1, 2, 1, 2, 1, 2, 3, 3, 3, 3, 1, 2, 1, 2, 1, 2, 1, 2, 3, 3, 3, 3, 1, 1, 1, 2, 1, 2, 2, 3,
    2, 3, 3, 3, 1, 1, 1, 1, 2, 2, 2, 3, 2, 3, 3, 3)
NT = (((1,), (1,)), ((), ()))


def arrival_orders(n):
    orders = []
    for z in range(n):
        first = 1 if z < n / 2 else -1
        order = [z]
        for d in range(1, n):
            order += [b for b in (z + first * d, z - first * d) if 0 <= b < n]
        orders.append(order)
    return orders


def stream_plan(n, layers):
    ms = 2 * layers
    edge = [(m, s, q) for m in range(ms) for s in range(1, n) for q in range(PIECES)]
    seen = [0] * n
    inner = []
    for s in INNER_ORDER:
        inner.append((seen[s] // PIECES, s, seen[s] % PIECES))
        seen[s] += 1
    return edge, inner


def mean_and_scale(stats):
    mean = stats[0:1, :]
    inv = lax.rsqrt(stats[1:2, :] - mean * mean + EPSILON)
    row = lax.broadcasted_iota(jnp.int32, (128, stats.shape[1]), 0)
    cols = jnp.where(row == 0, mean, jnp.where(row == 1, inv, 0.0)).T
    return cols[:, 0:1], cols[:, 1:2]


def finish(d_model, last, summed, totals_in, gain_in, shift_in, out,
           held, ready, totals, norm_gain, norm_shift, in_sem, out_sem, side_sem):
    tokens = held.shape[0]
    size = 256 if tokens % 256 == 0 else 128
    blocks = [pl.ds(i * size, size) for i in range(tokens // size)]
    loads = [pltpu.make_async_copy(summed.at[r], held.at[r], in_sem.at[i]) for i, r in enumerate(blocks)]
    stores = [pltpu.make_async_copy(ready.at[r], out.at[r], out_sem.at[i]) for i, r in enumerate(blocks)]
    sides = [pltpu.make_async_copy(a, b, side_sem.at[i]) for i, (a, b) in enumerate(
        ((totals_in, totals), (gain_in, norm_gain), (shift_in, norm_shift)))]
    for load in sides + loads:
        load.start()
    for side in sides:
        side.wait()
    for i, r in enumerate(blocks):
        mean, inv = mean_and_scale(totals[:, i * size:(i + 1) * size] / d_model)
        loads[i].wait()
        v = (held[r, :] - mean) * inv
        ready[r, :] = (v * norm_gain[last:last + 1, :] + norm_shift[last:last + 1, :]).astype(BF16)
        stores[i].start()
    for store in stores:
        store.wait()


def kernel(cfg, *refs):
    n, tp_n, layers, groups, width, streamed = cfg
    (stream, w_in, w_out, mix_in, gain_in, norm_gain_in, norm_shift_in, out, totals_out,
     mix, gain, norm_gain, norm_shift, wg, cur, acc, psend, precv, pown, xsend, xrecv, hbuf, sc, tsend, trecv, esend, erecv,
     loc_sem, stream_send, z_recv, y_recv,
     p_send_s, p_recv_s, x_send_s, x_recv_s, halo_s,
     c_send_s, c_recv_s, t_send_s, t_recv_s, e_send_s, e_recv_s, out_sem) = refs
    tokens, chans = stream.shape
    half = tokens // 2
    halo = layers * REACH
    ahead = halo - REACH
    reach_rows = half + halo
    part_rows = half + ahead
    d_model = chans * tp_n
    alpha = (2.0 * layers) ** 0.25
    nx = tp_n // 2
    y, z, t = lax.axis_index("grp"), lax.axis_index("sp"), lax.axis_index("tp")
    core, x = lax.rem(t, 2), t // 2
    sib = t + 1 - 2 * core
    orders = arrival_orders(n)
    mine, other = core * half, (1 - core) * half
    mine = pl.multiple_of(mine, REACH)
    other = pl.multiple_of(other, REACH)

    def order(s):
        if not streamed:
            return jnp.int32(s)
        b = jnp.int32(0)
        for k in range(n):
            b = jnp.where(z == k, orders[k][s], b)
        return b

    def remote(src, dst, ssem, rsem, device):
        return pltpu.make_async_remote_copy(
            src_ref=src, dst_ref=dst, send_sem=ssem, recv_sem=rsem,
            device_id=device, device_id_type=MESH)

    barrier = pltpu.get_barrier_semaphore()

    def greet(device):
        pl.semaphore_signal(barrier, inc=1, device_id=device, device_id_type=MESH)

    for k in range(1, tp_n):
        greet((y, z, lax.rem(t + k, tp_n)))
    count = jnp.int32(tp_n - 1)
    if streamed:
        greet((1 - y, z, t))
        count = count + 1

    @pl.when(z > 0)
    def _():
        greet((y, z - 1, t))

    @pl.when(z < n - 1)
    def _():
        greet((y, z + 1, t))

    count = count + jnp.where(z > 0, 1, 0) + jnp.where(z < n - 1, 1, 0)
    rows = w_in.shape[1]
    copies = [pltpu.make_async_copy(stream, cur.at[pl.ds(halo, tokens)], loc_sem.at[0])]
    for m in range(2 * layers):
        src = (w_in, w_out)[m % 2].at[m // 2]
        if streamed:
            dst = wg.at[m, pl.ds(pl.multiple_of(z * rows, rows), rows)]
        else:
            dst = wg.at[m]
        copies.append(pltpu.make_async_copy(src, dst, loc_sem.at[1 + m]))
    for at, pair in enumerate(((mix_in, mix), (gain_in, gain), (norm_gain_in, norm_gain), (norm_shift_in, norm_shift))):
        copies.append(pltpu.make_async_copy(*pair, loc_sem.at[1 + 2 * layers + at]))
    for copy in copies:
        copy.start()

    pl.semaphore_wait(barrier, count)

    part = rows // 2
    cut = part // PIECES

    def span(base, q):
        return pl.ds(pl.multiple_of(base + q * cut, cut), cut)

    edge = (z == 0) | (z == n - 1)

    def place(b, zt):
        return b - jnp.where(b > zt, 1, 0)

    def own_copy(m, side, q):
        src = (w_in, w_out)[m % 2].at[m // 2, span(y * part, q)]
        dst = wg.at[m, span(z * rows + y * part, q)]
        zt = z + 2 * side - 1
        return remote(src, dst, stream_send.at[0], z_recv.at[m, place(z, zt), q], (y, zt, t))

    def rest_copy(m, q):
        src = (w_in, w_out)[m % 2].at[m // 2, span((1 - y) * part, q)]
        dst = wg.at[m, span(z * rows + (1 - y) * part, q)]
        return remote(src, dst, stream_send.at[0], y_recv.at[m, z],
                      (y, jnp.where(z == 0, 1, n - 2), t))

    def own_start(m, k, side):
        if not 0 <= k + 2 * side - 1 < n:
            return

        @pl.when(z == k)
        def _():
            for q in range(PIECES):
                own_copy(m, side, q).start()
            if m == 0 and side:
                halo_copy().start()
            if k in (0, n - 1):
                for q in range(PIECES):
                    rest_copy(m, q).start()

    def arrived(m, b, q):
        ref = wg.at[m, span(b * rows + y * part, q)]
        remote(ref, ref, stream_send.at[0], z_recv.at[m, place(b, z), q], (y, z, t)).wait_recv()

    def onward(m, b, q):
        zt = jnp.where(b < z, z + 1, z - 1)
        ref = wg.at[m, span(b * rows + y * part, q)]
        return (zt >= 0) & (zt < n), remote(
            ref, ref, stream_send.at[0], z_recv.at[m, place(b, zt), q], (y, zt, t))

    def whole(b):
        return ((z == 1) & (b == 0)) | ((z == n - 2) & (b == n - 1))

    def across(m, b, from_y, q):
        ref = wg.at[m, span(b * rows + from_y * part, q)]
        return remote(ref, ref, stream_send.at[0], y_recv.at[m, b], (1 - y, z, t))

    def by_place(values):
        picked = jnp.int32(values[0])
        for k in range(1, n):
            if values[k] != values[0]:
                picked = jnp.where(z == k, values[k], picked)
        return picked

    edge_events, inner_events = stream_plan(n, layers)
    state = [0, 0]

    def take(e_event, i_event):
        places = [k for k in range(n) if (e_event if k in (0, n - 1) else i_event)]

        def go():
            vals = [(e_event if k in (0, n - 1) else i_event) or e_event or i_event for k in range(n)]
            m = by_place([v[0] for v in vals])
            b = by_place([orders[k][v[1]] for k, v in enumerate(vals)])
            q = by_place([v[2] for v in vals])
            there, copy = onward(m, b, q)
            arrived(m, b, q)
            pl.when(there)(copy.start)
            pl.when(jnp.logical_not(whole(b)))(across(m, b, y, q).start)

        if len(places) == n:
            go()
        else:
            pl.when(edge if e_event else jnp.logical_not(edge))(go)
        for k in places:
            m, s, q = e_event if k in (0, n - 1) else i_event
            if q != PIECES - 1 or m + 1 >= 2 * layers:
                continue
            if k in (0, n - 1):
                if s == 1:
                    own_start(m + 1, k, 1 if k == 0 else 0)
            elif s == n - 1:
                own_start(m + 1, k, 0 if k < n / 2 else 1)
            elif s == 2:
                own_start(m + 1, k, 1 if k < n / 2 else 0)

    def tick(e_goal, i_goal):
        if not streamed:
            return
        while state[0] < e_goal or state[1] < i_goal:
            e_event = i_event = None
            if state[0] < e_goal:
                e_event = edge_events[state[0]]
                state[0] += 1
            if state[1] < i_goal:
                i_event = inner_events[state[1]]
                state[1] += 1
            take(e_event, i_event)

    def ready(m, s):
        if s == 0:
            copies[1 + m].wait()
        elif streamed:
            b = order(s)
            ref = wg.at[m, pl.ds(pl.multiple_of(b * rows + (1 - y) * part, part), part)]
            remote(ref, ref, stream_send.at[0], y_recv.at[m, b], (y, z, t)).wait_recv()

    def weight(m, s):
        return wg[m, pl.ds(pl.multiple_of(order(s) * width, width), width), :]

    def p_copy(l, s):
        return remote(psend.at[l, s], precv.at[l, s], p_send_s.at[0], p_recv_s.at[l, s], (y, z, sib))

    def x_copies(l, s):
        return [remote(xsend.at[l, s], xrecv.at[k - 1, l, s], x_send_s.at[0],
                       x_recv_s.at[k - 1, l, s], (y, z, lax.rem(x + k, nx) * 2 + core))
                for k in range(1, nx)]

    def halo_copy():
        return remote(stream.at[pl.ds(tokens - halo, halo)], cur.at[pl.ds(0, halo)],
                      halo_s.at[0], halo_s.at[1], (y, jnp.minimum(z + 1, n - 1), t))

    def c_copy(l, s, side):
        ref = sc.at[l, s, side]
        return remote(ref, ref, c_send_s.at[0], c_recv_s.at[l, s], (y, z, sib))

    def t_copies(l, i):
        return [remote(tsend.at[l, i], trecv.at[k - 1, l, i], t_send_s.at[0],
                       t_recv_s.at[l, i], (y, z, lax.rem(t + k, tp_n)))
                for k in range(1, tp_n)]

    def e_copies(l):
        return [remote(esend.at[l], erecv.at[k - 1, l], e_send_s.at[0],
                       e_recv_s.at[l], (y, z, lax.rem(t + k, tp_n)))
                for k in range(1, tp_n)]

    def settle(ref, sem):
        pltpu.make_async_copy(ref, ref, sem).wait()

    def project(l, s):
        w = weight(2 * l, s)
        psend[l, s] = lax.dot_general(
            cur[pl.ds(other, reach_rows), :], w, NT, preferred_element_type=F32).astype(BF16)
        p_copy(l, s).start()
        pown[s] = lax.dot_general(cur[pl.ds(mine, reach_rows), :], w, NT, preferred_element_type=F32)

    def chip_sum(l, s):
        p_copy(l, s).wait_recv()
        total = pown[s] + precv[l, s].astype(F32)
        pown[s] = total
        xsend[l, s] = total.astype(BF16)
        for copy in x_copies(l, s):
            copy.start()

    def finish_hidden(l, s):
        total = pown[s]
        for k, copy in enumerate(x_copies(l, s)):
            copy.wait_recv()
            total = total + xrecv[k, l, s].astype(F32)
        hbuf[s] = total.astype(BF16).astype(F32)

        @pl.when((z == 0) & (core == 0))
        def _():
            hbuf[s, :halo, :] = jnp.zeros((halo, width), F32)

    def pool(l, s):
        b = order(s)
        ext = hbuf[s]
        run = ext + pltpu.roll(ext, 1, 0)
        for octave in range(1, groups):
            take = jnp.where(b >= octave, 1.0, 0.0).astype(F32)
            run = run + take * pltpu.roll(run, 2**octave, 0)
        reach = jnp.int32(2)
        for octave in range(1, groups):
            reach = jnp.where(b >= octave, 2 ** (octave + 1), reach)
        at = z * tokens + core * half - ahead + 1 + lax.broadcasted_iota(jnp.int32, (part_rows, width), 0)
        counts = jnp.clip(at, 1, reach).astype(F32)
        pooled = (run[REACH:, :] / counts - ext[REACH:, :]).astype(BF16)
        mixed = jnp.dot(pooled, mix[l, b], preferred_element_type=F32)
        sc[l, s, core] = (mixed * gain[l:l + 1, pl.ds(pl.multiple_of(b * width, width), width)]).astype(BF16)
        c_copy(l, s, core).start()

    def grow(l, s, add, rows_at, cur_at):
        if s == 0:
            acc[rows_at, :] = alpha * cur[cur_at, :].astype(F32) + add
        else:
            acc[rows_at, :] = acc[rows_at, :] + add

    def row_totals(v):
        lane = lax.broadcasted_iota(jnp.int32, (v.shape[0], 128), 1)
        row_sum = jnp.sum(v, axis=1, keepdims=True)
        row_squares = jnp.sum(v * v, axis=1, keepdims=True)
        return jnp.where(lane == 0, row_sum, jnp.where(lane == 1, row_squares, 0.0))

    def expand(l, s):
        c_copy(l, s, 1 - core).wait_recv()
        at_m = 2 * l + 1
        extra = l * REACH

        if extra < ahead:
            add = jnp.dot(sc[l, s, 0, extra:ahead, :], weight(at_m, s), preferred_element_type=F32)
            grow(l, s, add, slice(extra, ahead), slice(extra + REACH, halo))
            if s == groups - 1:
                esend[l, extra:, :] = row_totals(acc[extra:ahead, :])
                for copy in e_copies(l):
                    copy.start()

        def body(i, carry):
            add = jnp.dot(sc[l, s, i, ahead:, :], weight(at_m, s), preferred_element_type=F32)
            at = i * half
            if not isinstance(i, int):
                at = pl.multiple_of(at, REACH)
            grow(l, s, add, pl.ds(ahead + at, half), pl.ds(halo + at, half))
            return carry

        if s < groups - 1:
            lax.fori_loop(0, 2, body, 0)
            return
        for i in range(2):
            body(i, 0)
            both = row_totals(acc[ahead + i * half:ahead + (i + 1) * half, :])
            tsend[l, i] = both.T[:8, :]
            for copy in t_copies(l, i):
                copy.start()
            if l == layers - 1:
                out_copy(i).start()

    def out_copy(i):
        return pltpu.make_async_copy(
            acc.at[pl.ds(ahead + i * half, half)], out.at[pl.ds(i * half, half)], out_sem.at[i])

    def norm(l, i):
        extra = l * REACH

        def apply(at, mean, inv, size):
            v = (acc[at:at + size, :] - mean) * inv
            to = at - ahead + halo
            cur[to:to + size, :] = (v * norm_gain[l:l + 1, :] + norm_shift[l:l + 1, :]).astype(BF16)

        if extra < ahead and i == 0:
            stats = esend[l, extra:, :]
            settle(erecv.at[:, l], e_recv_s.at[l])
            for k in range(tp_n - 1):
                stats = stats + erecv[k, l, extra:, :]
            stats = stats / d_model
            mean = stats[:, 0:1]
            inv = lax.rsqrt(stats[:, 1:2] - mean * mean + EPSILON)
            apply(extra, mean, inv, ahead - extra)
        stats = tsend[l, i]
        settle(trecv.at[:, l, i], t_recv_s.at[l, i])
        for k in range(tp_n - 1):
            stats = stats + trecv[k, l, i]
        if l == layers - 1:
            totals_out[:, i * half:(i + 1) * half] = stats
            return
        apply(ahead + i * half, *mean_and_scale(stats / d_model), half)


    if streamed:
        for k in range(n):
            for side in (1, 0):
                own_start(0, k, side)
    else:
        pl.when(z < n - 1)(halo_copy().start)

    def before_first():
        @pl.when(z > 0)
        def _():
            halo_copy().wait_recv()

        @pl.when(z == 0)
        def _():
            cur[:halo, :] = jnp.zeros((halo, chans), BF16)

        copies[0].wait()
        for copy in copies[1 + 2 * layers:]:
            copy.wait()

    def drain():
        if streamed:
            @pl.when(edge)
            def _():
                settle(wg.at[:, pl.ds(0, (n + 1) * part)], stream_send.at[0])

            @pl.when(jnp.logical_not(edge))
            def _():
                settle(wg.at[:, pl.ds(0, (2 * n - 1) * part)], stream_send.at[0])
        settle(psend, p_send_s.at[0])
        if nx > 1:
            settle(xrecv, x_send_s.at[0])
        settle(sc.at[:, :, core], c_send_s.at[0])
        settle(trecv, t_send_s.at[0])
        settle(erecv.at[:, pl.ds(0, layers - 1)], e_send_s.at[0])
        pl.when(z < n - 1)(halo_copy().wait_send)

    phases = {"project": project, "chip_sum": chip_sum, "finish_hidden": finish_hidden,
              "pool": pool, "expand": expand, "norm": norm}
    at = 0
    for l in range(layers):
        for name, s in STEPS:
            if at < len(EDGE_TICKS):
                tick(EDGE_TICKS[at], INNER_TICKS[at])
            if at == 0:
                before_first()
            if name == "project":
                ready(2 * l, s)
            elif name == "expand":
                ready(2 * l + 1, s)
            phases[name](l, s)
            at += 1

    drain()
    for i in range(2):
        out_copy(i).wait()


def per_device(n, grp_n, tp_n, stream, in_weight, out_weight, group_mix, pool_gain, norm_gain, norm_shift):
    layers, groups, width = group_mix.shape[:3]
    tokens, chans = stream.shape
    pool = groups * width
    streamed = n == groups == 4 and grp_n == 2 and layers == 2
    if not streamed:
        in_weight = lax.all_gather(in_weight, "sp", axis=1, tiled=True)
        out_weight = lax.all_gather(out_weight, "sp", axis=1, tiled=True)
    nx = tp_n // 2
    half = tokens // 2
    halo = layers * REACH
    ahead = halo - REACH
    ms = 2 * layers
    dma = pltpu.SemaphoreType.DMA
    any_spec = pl.BlockSpec(memory_space=pl.ANY)
    vmem = pl.BlockSpec(memory_space=pltpu.VMEM)
    xs = max(nx - 1, 1)
    summed, totals = pl.pallas_call(
        functools.partial(kernel, (n, tp_n, layers, groups, width, streamed)),
        out_shape=(jax.ShapeDtypeStruct((tokens, chans), F32), jax.ShapeDtypeStruct((8, tokens), F32)),
        in_specs=[any_spec] * 7,
        out_specs=(any_spec, vmem),
        scratch_shapes=[
            pltpu.VMEM(group_mix.shape, BF16),
            pltpu.VMEM(pool_gain.shape, F32),
            pltpu.VMEM(norm_gain.shape, F32),
            pltpu.VMEM(norm_shift.shape, F32),
            pltpu.VMEM((ms, pool, chans), BF16),
            pltpu.VMEM((halo + tokens, chans), BF16),
            pltpu.VMEM((ahead + tokens, chans), F32),
            pltpu.VMEM((layers, groups, halo + half, width), BF16),
            pltpu.VMEM((layers, groups, halo + half, width), BF16),
            pltpu.VMEM((groups, halo + half, width), F32),
            pltpu.VMEM((layers, groups, halo + half, width), BF16),
            pltpu.VMEM((xs, layers, groups, halo + half, width), BF16),
            pltpu.VMEM((groups, halo + half, width), F32),
            pltpu.VMEM((layers, groups, 2, ahead + half, width), BF16),
            pltpu.VMEM((layers, 2, 8, half), F32),
            pltpu.VMEM((tp_n - 1, layers, 2, 8, half), F32),
            pltpu.VMEM((layers, ahead, 128), F32),
            pltpu.VMEM((tp_n - 1, layers, ahead, 128), F32),
            dma((5 + ms,)),
            dma((1,)), dma((ms, groups - 1, PIECES)), dma((ms, groups)),
            dma((1,)), dma((layers, groups)),
            dma((1,)), dma((xs, layers, groups)),
            dma((2,)),
            dma((1,)), dma((layers, groups)),
            dma((1,)), dma((layers, 2)),
            dma((1,)), dma((layers,)),
            dma((2,)),
        ],
        compiler_params=pltpu.CompilerParams(
            collective_id=0, has_side_effects=True, vmem_limit_bytes=56 * 1024 * 1024),
    )(stream, in_weight, out_weight, group_mix,
      pool_gain, norm_gain, norm_shift)
    steps = tokens // (256 if tokens % 256 == 0 else 128)
    return pl.pallas_call(
        functools.partial(finish, chans * tp_n, layers - 1),
        out_shape=jax.ShapeDtypeStruct((tokens, chans), BF16),
        in_specs=[any_spec] * 4,
        out_specs=any_spec,
        scratch_shapes=[
            pltpu.VMEM((tokens, chans), F32),
            pltpu.VMEM((tokens, chans), BF16),
            pltpu.VMEM((8, tokens), F32),
            pltpu.VMEM(norm_gain.shape, F32),
            pltpu.VMEM(norm_shift.shape, F32),
            dma((steps,)),
            dma((steps,)),
            dma((3,)),
        ],
    )(summed, totals, norm_gain, norm_shift)


def solution(mesh):
    in_specs = (
        P(("grp", "sp"), "tp"),
        P(None, "sp", "tp"),
        P(None, "sp", "tp"),
        P(),
        P(),
        P(None, "tp"),
        P(None, "tp"),
    )
    out_specs = P(("grp", "sp"), "tp")
    sizes = mesh.shape
    body = functools.partial(per_device, sizes["sp"], sizes["grp"], sizes["tp"])
    return jax.shard_map(
        body, mesh=mesh, in_specs=in_specs, out_specs=out_specs, check_vma=False
    )
```

```python
import functools

import jax
import jax.numpy as jnp
from jax import lax
from jax.experimental import pallas as pl
from jax.experimental.pallas import tpu as pltpu
from jax.sharding import PartitionSpec as P

MESH = pl.DeviceIdType.MESH
EPSILON = 1e-05
F32 = jnp.float32
BF16 = jnp.bfloat16
REACH = 16
PIECES = 4
GIFT = 2
STEPS = (
    ("project", 0), ("chip_sum", 0), ("project", 1), ("chip_sum", 1), ("project", 2), ("chip_sum",
    2), ("project", 3), ("chip_sum", 3), ("finish_hidden", 0), ("pool", 0), ("finish_hidden", 1),
    ("pool", 1), ("expand", 0), ("finish_hidden", 2), ("pool", 2), ("expand", 1), ("finish_hidden",
    3), ("pool", 3), ("expand", 2), ("expand", 3), ("norm", 0), ("norm", 1),
)
EDGE_TICKS = (4, 6, 7, 9, 11, 13, 15, 17, 17, 17, 17, 17, 18, 19, 19, 19, 22, 22, 23, 27, 29, 30, 30, 32, 32,
    33, 35, 37, 39, 41, 41, 41, 41, 41, 42, 43, 43, 44, 47, 47, 47, 48, 48, 48)
INNER_TICKS = (8, 10, 11, 12, 12, 16, 18, 20, 20, 20, 22, 22, 22, 25, 25, 26, 30, 30, 31, 33, 35, 35, 35, 37,
    37, 38, 38, 40, 40, 40, 41, 41, 45, 45, 46, 48, 48, 48, 48, 48, 48, 48, 48, 48)
INNER_ORDER = (1, 2, 1, 2, 1, 2, 1, 2, 3, 3, 3, 3, 1, 2, 1, 2, 1, 2, 1, 2, 3, 3, 3, 3, 1, 1, 1, 2, 1, 2, 2, 3,
    2, 3, 3, 3, 1, 1, 1, 1, 2, 2, 2, 3, 2, 3, 3, 3)
NT = (((1,), (1,)), ((), ()))


def arrival_orders(n):
    orders = []
    for z in range(n):
        first = 1 if z < n / 2 else -1
        order = [z]
        for d in range(1, n):
            order += [b for b in (z + first * d, z - first * d) if 0 <= b < n]
        orders.append(order)
    return orders


def stream_plan(n, layers):
    ms = 2 * layers
    edge = [(m, s, q) for m in range(ms) for s in range(1, n) for q in range(PIECES)]
    seen = [0] * n
    inner = []
    for s in INNER_ORDER:
        inner.append((seen[s] // PIECES, s, seen[s] % PIECES))
        seen[s] += 1
    return edge, inner


def mean_and_scale(stats):
    mean = stats[0:1, :]
    inv = lax.rsqrt(stats[1:2, :] - mean * mean + EPSILON)
    row = lax.broadcasted_iota(jnp.int32, (128, stats.shape[1]), 0)
    cols = jnp.where(row == 0, mean, jnp.where(row == 1, inv, 0.0)).T
    return cols[:, 0:1], cols[:, 1:2]


def finish(d_model, last, summed, totals_in, gain_in, shift_in, out,
           held, ready, totals, norm_gain, norm_shift, in_sem, out_sem, side_sem):
    tokens = held.shape[0]
    size = 256 if tokens % 256 == 0 else 128
    blocks = [pl.ds(i * size, size) for i in range(tokens // size)]
    loads = [pltpu.make_async_copy(summed.at[r], held.at[r], in_sem.at[i]) for i, r in enumerate(blocks)]
    stores = [pltpu.make_async_copy(ready.at[r], out.at[r], out_sem.at[i]) for i, r in enumerate(blocks)]
    sides = [pltpu.make_async_copy(a, b, side_sem.at[i]) for i, (a, b) in enumerate(
        ((totals_in, totals), (gain_in, norm_gain), (shift_in, norm_shift)))]
    for load in sides + loads:
        load.start()
    for side in sides:
        side.wait()
    for i, r in enumerate(blocks):
        mean, inv = mean_and_scale(totals[:, i * size:(i + 1) * size] / d_model)
        loads[i].wait()
        v = (held[r, :] - mean) * inv
        ready[r, :] = (v * norm_gain[last:last + 1, :] + norm_shift[last:last + 1, :]).astype(BF16)
        stores[i].start()
    for store in stores:
        store.wait()


def kernel(cfg, *refs):
    n, tp_n, layers, groups, width, streamed = cfg
    (stream, w_in, w_out, mix_in, gain_in, norm_gain_in, norm_shift_in, out, totals_out,
     mix, gain, norm_gain, norm_shift, wg, cur, acc, psend, precv, pown, xsend, xrecv, hbuf, sc, tsend, trecv, esend, erecv,
     loc_sem, stream_send, z_recv, y_recv,
     p_send_s, p_recv_s, x_send_s, x_recv_s, halo_s,
     c_send_s, c_recv_s, t_send_s, t_recv_s, e_send_s, e_recv_s, out_sem) = refs
    tokens, chans = stream.shape
    half = tokens // 2
    halo = layers * REACH
    ahead = halo - REACH
    reach_rows = half + halo
    part_rows = half + ahead
    d_model = chans * tp_n
    alpha = (2.0 * layers) ** 0.25
    nx = tp_n // 2
    y, z, t = lax.axis_index("grp"), lax.axis_index("sp"), lax.axis_index("tp")
    core, x = lax.rem(t, 2), t // 2
    sib = t + 1 - 2 * core
    orders = arrival_orders(n)
    mine, other = core * half, (1 - core) * half
    mine = pl.multiple_of(mine, REACH)
    other = pl.multiple_of(other, REACH)

    def order(s):
        if not streamed:
            return jnp.int32(s)
        b = jnp.int32(0)
        for k in range(n):
            b = jnp.where(z == k, orders[k][s], b)
        return b

    def remote(src, dst, ssem, rsem, device):
        return pltpu.make_async_remote_copy(
            src_ref=src, dst_ref=dst, send_sem=ssem, recv_sem=rsem,
            device_id=device, device_id_type=MESH)

    barrier = pltpu.get_barrier_semaphore()

    def greet(device):
        pl.semaphore_signal(barrier, inc=1, device_id=device, device_id_type=MESH)

    for k in range(1, tp_n):
        greet((y, z, lax.rem(t + k, tp_n)))
    count = jnp.int32(tp_n - 1)
    if streamed:
        greet((1 - y, z, t))
        count = count + 1

    @pl.when(z > 0)
    def _():
        greet((y, z - 1, t))

    @pl.when(z < n - 1)
    def _():
        greet((y, z + 1, t))

    count = count + jnp.where(z > 0, 1, 0) + jnp.where(z < n - 1, 1, 0)
    rows = w_in.shape[1]
    copies = [pltpu.make_async_copy(stream, cur.at[pl.ds(halo, tokens)], loc_sem.at[0])]
    for m in range(2 * layers):
        src = (w_in, w_out)[m % 2].at[m // 2]
        if streamed:
            dst = wg.at[m, pl.ds(pl.multiple_of(z * rows, rows), rows)]
        else:
            dst = wg.at[m]
        copies.append(pltpu.make_async_copy(src, dst, loc_sem.at[1 + m]))
    for at, pair in enumerate(((mix_in, mix), (gain_in, gain), (norm_gain_in, norm_gain), (norm_shift_in, norm_shift))):
        copies.append(pltpu.make_async_copy(*pair, loc_sem.at[1 + 2 * layers + at]))
    for copy in copies:
        copy.start()

    pl.semaphore_wait(barrier, count)

    part = rows // 2
    cut = part // PIECES

    def span(base, q):
        return pl.ds(pl.multiple_of(base + q * cut, cut), cut)

    edge = (z == 0) | (z == n - 1)

    def place(b, zt):
        return b - jnp.where(b > zt, 1, 0)

    def own_copy(m, side, q):
        src = (w_in, w_out)[m % 2].at[m // 2, span(y * part, q)]
        dst = wg.at[m, span(z * rows + y * part, q)]
        zt = z + 2 * side - 1
        return remote(src, dst, stream_send.at[0], z_recv.at[m, place(z, zt), q], (y, zt, t))

    def rest_copy(m, q):
        src = (w_in, w_out)[m % 2].at[m // 2, span((1 - y) * part, q)]
        dst = wg.at[m, span(z * rows + (1 - y) * part, q)]
        return remote(src, dst, stream_send.at[0], y_recv.at[m, z],
                      (y, jnp.where(z == 0, 1, n - 2), t))

    def own_start(m, k, side):
        if not 0 <= k + 2 * side - 1 < n:
            return

        @pl.when(z == k)
        def _():
            for q in range(PIECES):
                own_copy(m, side, q).start()
            if m == 0 and side:
                halo_copy().start()
            if k in (0, n - 1):
                for q in range(PIECES):
                    rest_copy(m, q).start()

    def arrived(m, b, q):
        ref = wg.at[m, span(b * rows + y * part, q)]
        remote(ref, ref, stream_send.at[0], z_recv.at[m, place(b, z), q], (y, z, t)).wait_recv()

    def onward(m, b, q):
        zt = jnp.where(b < z, z + 1, z - 1)
        ref = wg.at[m, span(b * rows + y * part, q)]
        return (zt >= 0) & (zt < n), remote(
            ref, ref, stream_send.at[0], z_recv.at[m, place(b, zt), q], (y, zt, t))

    def whole(b):
        return ((z == 1) & (b == 0)) | ((z == n - 2) & (b == n - 1))

    def across(m, b, from_y, q):
        ref = wg.at[m, span(b * rows + from_y * part, q)]
        return remote(ref, ref, stream_send.at[0], y_recv.at[m, b], (1 - y, z, t))

    def by_place(values):
        picked = jnp.int32(values[0])
        for k in range(1, n):
            if values[k] != values[0]:
                picked = jnp.where(z == k, values[k], picked)
        return picked

    edge_events, inner_events = stream_plan(n, layers)
    state = [0, 0]

    def take(e_event, i_event):
        places = [k for k in range(n) if (e_event if k in (0, n - 1) else i_event)]

        def go():
            vals = [(e_event if k in (0, n - 1) else i_event) or e_event or i_event for k in range(n)]
            m = by_place([v[0] for v in vals])
            b = by_place([orders[k][v[1]] for k, v in enumerate(vals)])
            q = by_place([v[2] for v in vals])
            there, copy = onward(m, b, q)
            arrived(m, b, q)
            pl.when(there)(copy.start)
            given = edge & (m == 2 * layers - 1) & (b == n - 1 - z) & (q >= PIECES - GIFT)
            pl.when(jnp.logical_not(whole(b) | given))(across(m, b, y, q).start)

        if len(places) == n:
            go()
        else:
            pl.when(edge if e_event else jnp.logical_not(edge))(go)
        for k in places:
            m, s, q = e_event if k in (0, n - 1) else i_event
            if q != PIECES - 1 or m + 1 >= 2 * layers:
                continue
            if k in (0, n - 1):
                if s == 1:
                    own_start(m + 1, k, 1 if k == 0 else 0)
            elif s == n - 1:
                own_start(m + 1, k, 0 if k < n / 2 else 1)
            elif s == 2:
                own_start(m + 1, k, 1 if k < n / 2 else 0)

    def tick(e_goal, i_goal):
        if not streamed:
            return
        while state[0] < e_goal or state[1] < i_goal:
            e_event = i_event = None
            if state[0] < e_goal:
                e_event = edge_events[state[0]]
                state[0] += 1
            if state[1] < i_goal:
                i_event = inner_events[state[1]]
                state[1] += 1
            take(e_event, i_event)

    def ready(m, s):
        if s == 0:
            copies[1 + m].wait()
        elif streamed:
            b = order(s)
            ref = wg.at[m, pl.ds(pl.multiple_of(b * rows + (1 - y) * part, part), part)]
            remote(ref, ref, stream_send.at[0], y_recv.at[m, b], (y, z, t)).wait_recv()

    def weight(m, s):
        return wg[m, pl.ds(pl.multiple_of(order(s) * width, width), width), :]

    def p_copy(l, s):
        return remote(psend.at[l, s], precv.at[l, s], p_send_s.at[0], p_recv_s.at[l, s], (y, z, sib))

    def x_copies(l, s):
        return [remote(xsend.at[l, s], xrecv.at[k - 1, l, s], x_send_s.at[0],
                       x_recv_s.at[k - 1, l, s], (y, z, lax.rem(x + k, nx) * 2 + core))
                for k in range(1, nx)]

    def halo_copy():
        return remote(stream.at[pl.ds(tokens - halo, halo)], cur.at[pl.ds(0, halo)],
                      halo_s.at[0], halo_s.at[1], (y, jnp.minimum(z + 1, n - 1), t))

    def c_copy(l, s, side):
        ref = sc.at[l, s, side]
        return remote(ref, ref, c_send_s.at[0], c_recv_s.at[l, s], (y, z, sib))

    def t_copies(l, i):
        return [remote(tsend.at[l, i], trecv.at[k - 1, l, i], t_send_s.at[0],
                       t_recv_s.at[l, i], (y, z, lax.rem(t + k, tp_n)))
                for k in range(1, tp_n)]

    def e_copies(l):
        return [remote(esend.at[l], erecv.at[k - 1, l], e_send_s.at[0],
                       e_recv_s.at[l], (y, z, lax.rem(t + k, tp_n)))
                for k in range(1, tp_n)]

    def settle(ref, sem):
        pltpu.make_async_copy(ref, ref, sem).wait()

    def project(l, s):
        w = weight(2 * l, s)
        psend[l, s] = lax.dot_general(
            cur[pl.ds(other, reach_rows), :], w, NT, preferred_element_type=F32).astype(BF16)
        p_copy(l, s).start()
        pown[s] = lax.dot_general(cur[pl.ds(mine, reach_rows), :], w, NT, preferred_element_type=F32)

    def chip_sum(l, s):
        p_copy(l, s).wait_recv()
        total = pown[s] + precv[l, s].astype(F32)
        pown[s] = total
        xsend[l, s] = total.astype(BF16)
        for copy in x_copies(l, s):
            copy.start()

    def finish_hidden(l, s):
        total = pown[s]
        for k, copy in enumerate(x_copies(l, s)):
            copy.wait_recv()
            total = total + xrecv[k, l, s].astype(F32)
        hbuf[s] = total.astype(BF16).astype(F32)

        @pl.when((z == 0) & (core == 0))
        def _():
            hbuf[s, :halo, :] = jnp.zeros((halo, width), F32)

    def pool(l, s):
        b = order(s)
        ext = hbuf[s]
        run = ext + pltpu.roll(ext, 1, 0)
        for octave in range(1, groups):
            take = jnp.where(b >= octave, 1.0, 0.0).astype(F32)
            run = run + take * pltpu.roll(run, 2**octave, 0)
        reach = jnp.int32(2)
        for octave in range(1, groups):
            reach = jnp.where(b >= octave, 2 ** (octave + 1), reach)
        at = z * tokens + core * half - ahead + 1 + lax.broadcasted_iota(jnp.int32, (part_rows, width), 0)
        counts = jnp.clip(at, 1, reach).astype(F32)
        pooled = (run[REACH:, :] / counts - ext[REACH:, :]).astype(BF16)
        mixed = jnp.dot(pooled, mix[l, b], preferred_element_type=F32)
        sc[l, s, core] = (mixed * gain[l:l + 1, pl.ds(pl.multiple_of(b * width, width), width)]).astype(BF16)
        c_copy(l, s, core).start()

    def grow(l, s, add, rows_at, cur_at):
        if s == 0:
            acc[rows_at, :] = alpha * cur[cur_at, :].astype(F32) + add
        else:
            acc[rows_at, :] = acc[rows_at, :] + add

    def row_totals(v):
        lane = lax.broadcasted_iota(jnp.int32, (v.shape[0], 128), 1)
        row_sum = jnp.sum(v, axis=1, keepdims=True)
        row_squares = jnp.sum(v * v, axis=1, keepdims=True)
        return jnp.where(lane == 0, row_sum, jnp.where(lane == 1, row_squares, 0.0))

    def expand(l, s):
        c_copy(l, s, 1 - core).wait_recv()
        at_m = 2 * l + 1
        extra = l * REACH

        if extra < ahead:
            add = jnp.dot(sc[l, s, 0, extra:ahead, :], weight(at_m, s), preferred_element_type=F32)
            grow(l, s, add, slice(extra, ahead), slice(extra + REACH, halo))
            if s == groups - 1:
                esend[l, extra:, :] = row_totals(acc[extra:ahead, :])
                for copy in e_copies(l):
                    copy.start()

        def body(i, carry):
            add = jnp.dot(sc[l, s, i, ahead:, :], weight(at_m, s), preferred_element_type=F32)
            at = i * half
            if not isinstance(i, int):
                at = pl.multiple_of(at, REACH)
            grow(l, s, add, pl.ds(ahead + at, half), pl.ds(halo + at, half))
            return carry

        if s < groups - 1:
            lax.fori_loop(0, 2, body, 0)
            return
        for i in range(2):
            body(i, 0)
            both = row_totals(acc[ahead + i * half:ahead + (i + 1) * half, :])
            tsend[l, i] = both.T[:8, :]
            for copy in t_copies(l, i):
                copy.start()
            if l == layers - 1:
                out_copy(i).start()

    def out_copy(i):
        return pltpu.make_async_copy(
            acc.at[pl.ds(ahead + i * half, half)], out.at[pl.ds(i * half, half)], out_sem.at[i])

    def norm(l, i):
        extra = l * REACH

        def apply(at, mean, inv, size):
            v = (acc[at:at + size, :] - mean) * inv
            to = at - ahead + halo
            cur[to:to + size, :] = (v * norm_gain[l:l + 1, :] + norm_shift[l:l + 1, :]).astype(BF16)

        if extra < ahead and i == 0:
            stats = esend[l, extra:, :]
            settle(erecv.at[:, l], e_recv_s.at[l])
            for k in range(tp_n - 1):
                stats = stats + erecv[k, l, extra:, :]
            stats = stats / d_model
            mean = stats[:, 0:1]
            inv = lax.rsqrt(stats[:, 1:2] - mean * mean + EPSILON)
            apply(extra, mean, inv, ahead - extra)
        stats = tsend[l, i]
        settle(trecv.at[:, l, i], t_recv_s.at[l, i])
        for k in range(tp_n - 1):
            stats = stats + trecv[k, l, i]
        if l == layers - 1:
            totals_out[:, i * half:(i + 1) * half] = stats
            return
        apply(ahead + i * half, *mean_and_scale(stats / d_model), half)


    if streamed:
        for k in range(n):
            for side in (1, 0):
                own_start(0, k, side)
    else:
        pl.when(z < n - 1)(halo_copy().start)

    def before_first():
        @pl.when(z > 0)
        def _():
            halo_copy().wait_recv()

        @pl.when(z == 0)
        def _():
            cur[:halo, :] = jnp.zeros((halo, chans), BF16)

        copies[0].wait()
        for copy in copies[1 + 2 * layers:]:
            copy.wait()

    def gift():
        m = 2 * layers - 1
        zt = jnp.where(z == 1, 0, n - 1)

        @pl.when(jnp.logical_not(edge))
        def _():
            for q in range(PIECES - GIFT, PIECES):
                b = order(n - 1)
                ref = wg.at[m, span(b * rows + (1 - y) * part, q)]
                remote(ref, ref, stream_send.at[0], y_recv.at[m, b], (y, zt, t)).start()

    def drain():
        if streamed:
            given = GIFT * cut // (2 * layers)

            @pl.when(edge)
            def _():
                settle(wg.at[:, pl.ds(0, (n + 1) * part - given)], stream_send.at[0])

            @pl.when(jnp.logical_not(edge))
            def _():
                settle(wg.at[:, pl.ds(0, (2 * n - 1) * part + given)], stream_send.at[0])
        settle(psend, p_send_s.at[0])
        if nx > 1:
            settle(xrecv, x_send_s.at[0])
        settle(sc.at[:, :, core], c_send_s.at[0])
        settle(trecv, t_send_s.at[0])
        settle(erecv.at[:, pl.ds(0, layers - 1)], e_send_s.at[0])
        pl.when(z < n - 1)(halo_copy().wait_send)

    phases = {"project": project, "chip_sum": chip_sum, "finish_hidden": finish_hidden,
              "pool": pool, "expand": expand, "norm": norm}
    at = 0
    for l in range(layers):
        for name, s in STEPS:
            if at < len(EDGE_TICKS):
                tick(EDGE_TICKS[at], INNER_TICKS[at])
            if at == 0:
                before_first()
            if name == "project":
                ready(2 * l, s)
            elif name == "expand":
                ready(2 * l + 1, s)
                if streamed and l == layers - 1 and s == groups - 1:
                    gift()
            phases[name](l, s)
            at += 1

    drain()
    for i in range(2):
        out_copy(i).wait()


def per_device(n, grp_n, tp_n, stream, in_weight, out_weight, group_mix, pool_gain, norm_gain, norm_shift):
    layers, groups, width = group_mix.shape[:3]
    tokens, chans = stream.shape
    pool = groups * width
    streamed = n == groups == 4 and grp_n == 2 and layers == 2
    if not streamed:
        in_weight = lax.all_gather(in_weight, "sp", axis=1, tiled=True)
        out_weight = lax.all_gather(out_weight, "sp", axis=1, tiled=True)
    nx = tp_n // 2
    half = tokens // 2
    halo = layers * REACH
    ahead = halo - REACH
    ms = 2 * layers
    dma = pltpu.SemaphoreType.DMA
    any_spec = pl.BlockSpec(memory_space=pl.ANY)
    vmem = pl.BlockSpec(memory_space=pltpu.VMEM)
    xs = max(nx - 1, 1)
    summed, totals = pl.pallas_call(
        functools.partial(kernel, (n, tp_n, layers, groups, width, streamed)),
        out_shape=(jax.ShapeDtypeStruct((tokens, chans), F32), jax.ShapeDtypeStruct((8, tokens), F32)),
        in_specs=[any_spec] * 7,
        out_specs=(any_spec, vmem),
        scratch_shapes=[
            pltpu.VMEM(group_mix.shape, BF16),
            pltpu.VMEM(pool_gain.shape, F32),
            pltpu.VMEM(norm_gain.shape, F32),
            pltpu.VMEM(norm_shift.shape, F32),
            pltpu.VMEM((ms, pool, chans), BF16),
            pltpu.VMEM((halo + tokens, chans), BF16),
            pltpu.VMEM((ahead + tokens, chans), F32),
            pltpu.VMEM((layers, groups, halo + half, width), BF16),
            pltpu.VMEM((layers, groups, halo + half, width), BF16),
            pltpu.VMEM((groups, halo + half, width), F32),
            pltpu.VMEM((layers, groups, halo + half, width), BF16),
            pltpu.VMEM((xs, layers, groups, halo + half, width), BF16),
            pltpu.VMEM((groups, halo + half, width), F32),
            pltpu.VMEM((layers, groups, 2, ahead + half, width), BF16),
            pltpu.VMEM((layers, 2, 8, half), F32),
            pltpu.VMEM((tp_n - 1, layers, 2, 8, half), F32),
            pltpu.VMEM((layers, ahead, 128), F32),
            pltpu.VMEM((tp_n - 1, layers, ahead, 128), F32),
            dma((5 + ms,)),
            dma((1,)), dma((ms, groups - 1, PIECES)), dma((ms, groups)),
            dma((1,)), dma((layers, groups)),
            dma((1,)), dma((xs, layers, groups)),
            dma((2,)),
            dma((1,)), dma((layers, groups)),
            dma((1,)), dma((layers, 2)),
            dma((1,)), dma((layers,)),
            dma((2,)),
        ],
        compiler_params=pltpu.CompilerParams(
            collective_id=0, has_side_effects=True, vmem_limit_bytes=56 * 1024 * 1024),
    )(stream, in_weight, out_weight, group_mix,
      pool_gain, norm_gain, norm_shift)
    steps = tokens // (256 if tokens % 256 == 0 else 128)
    return pl.pallas_call(
        functools.partial(finish, chans * tp_n, layers - 1),
        out_shape=jax.ShapeDtypeStruct((tokens, chans), BF16),
        in_specs=[any_spec] * 4,
        out_specs=any_spec,
        scratch_shapes=[
            pltpu.VMEM((tokens, chans), F32),
            pltpu.VMEM((tokens, chans), BF16),
            pltpu.VMEM((8, tokens), F32),
            pltpu.VMEM(norm_gain.shape, F32),
            pltpu.VMEM(norm_shift.shape, F32),
            dma((steps,)),
            dma((steps,)),
            dma((3,)),
        ],
    )(summed, totals, norm_gain, norm_shift)


def solution(mesh):
    in_specs = (
        P(("grp", "sp"), "tp"),
        P(None, "sp", "tp"),
        P(None, "sp", "tp"),
        P(),
        P(),
        P(None, "tp"),
        P(None, "tp"),
    )
    out_specs = P(("grp", "sp"), "tp")
    sizes = mesh.shape
    body = functools.partial(per_device, sizes["sp"], sizes["grp"], sizes["tp"])
    return jax.shard_map(
        body, mesh=mesh, in_specs=in_specs, out_specs=out_specs, check_vma=False
    )
```

```python
import functools

import jax
import jax.numpy as jnp
from jax import lax
from jax.experimental import pallas as pl
from jax.experimental.pallas import tpu as pltpu
from jax.sharding import PartitionSpec as P

MESH = pl.DeviceIdType.MESH
EPSILON = 1e-05
F32 = jnp.float32
BF16 = jnp.bfloat16
REACH = 16
PIECES = 4
GIFT = 2
STEPS = (
    ("project", 0), ("chip_sum", 0), ("project", 1), ("chip_sum", 1), ("project", 2), ("chip_sum",
    2), ("project", 3), ("chip_sum", 3), ("finish_hidden", 0), ("pool", 0), ("finish_hidden", 1),
    ("pool", 1), ("expand", 0), ("finish_hidden", 2), ("pool", 2), ("expand", 1), ("finish_hidden",
    3), ("pool", 3), ("expand", 2), ("expand", 3), ("norm", 0), ("norm", 1),
)
EDGE_TICKS = (4, 6, 7, 9, 11, 13, 15, 17, 17, 17, 17, 17, 18, 19, 19, 19, 22, 22, 23, 27, 29, 30, 30, 32, 32,
    33, 35, 37, 39, 41, 41, 41, 41, 41, 42, 43, 43, 44, 47, 47, 47, 48, 48, 48)
INNER_TICKS = (8, 10, 11, 12, 12, 16, 18, 20, 20, 20, 22, 22, 22, 25, 25, 26, 30, 30, 31, 33, 35, 35, 35, 37,
    37, 38, 38, 40, 40, 40, 41, 41, 45, 45, 46, 48, 48, 48, 48, 48, 48, 48, 48, 48)
INNER_ORDER = (1, 2, 1, 2, 1, 2, 1, 2, 3, 3, 3, 3, 1, 2, 1, 2, 1, 2, 1, 2, 3, 3, 3, 3, 1, 1, 1, 2, 1, 2, 2, 3,
    2, 3, 3, 3, 1, 1, 1, 1, 2, 2, 2, 3, 2, 3, 3, 3)
NT = (((1,), (1,)), ((), ()))


def arrival_orders(n):
    orders = []
    for z in range(n):
        first = 1 if z < n / 2 else -1
        order = [z]
        for d in range(1, n):
            order += [b for b in (z + first * d, z - first * d) if 0 <= b < n]
        orders.append(order)
    return orders


def stream_plan(n, layers):
    ms = 2 * layers
    edge = [(m, s, q) for m in range(ms) for s in range(1, n) for q in range(PIECES)]
    seen = [0] * n
    inner = []
    for s in INNER_ORDER:
        inner.append((seen[s] // PIECES, s, seen[s] % PIECES))
        seen[s] += 1
    return edge, inner


def mean_and_scale(stats):
    mean = stats[0:1, :]
    inv = lax.rsqrt(stats[1:2, :] - mean * mean + EPSILON)
    row = lax.broadcasted_iota(jnp.int32, (128, stats.shape[1]), 0)
    cols = jnp.where(row == 0, mean, jnp.where(row == 1, inv, 0.0)).T
    return cols[:, 0:1], cols[:, 1:2]


def finish(d_model, last, summed, totals_in, gain_in, shift_in, out,
           held, ready, totals, norm_gain, norm_shift, in_sem, out_sem, side_sem):
    tokens = held.shape[0]
    size = 256 if tokens % 256 == 0 else 128
    blocks = [pl.ds(i * size, size) for i in range(tokens // size)]
    loads = [pltpu.make_async_copy(summed.at[r], held.at[r], in_sem.at[i]) for i, r in enumerate(blocks)]
    stores = [pltpu.make_async_copy(ready.at[r], out.at[r], out_sem.at[i]) for i, r in enumerate(blocks)]
    sides = [pltpu.make_async_copy(a, b, side_sem.at[i]) for i, (a, b) in enumerate(
        ((totals_in, totals), (gain_in, norm_gain), (shift_in, norm_shift)))]
    for load in sides + loads:
        load.start()
    for side in sides:
        side.wait()
    for i, r in enumerate(blocks):
        mean, inv = mean_and_scale(totals[:, i * size:(i + 1) * size] / d_model)
        loads[i].wait()
        v = (held[r, :] - mean) * inv
        ready[r, :] = (v * norm_gain[last:last + 1, :] + norm_shift[last:last + 1, :]).astype(BF16)
        stores[i].start()
    for store in stores:
        store.wait()


def kernel(cfg, *refs):
    n, tp_n, layers, groups, width, streamed = cfg
    (stream, w_in, w_out, mix_in, gain_in, norm_gain_in, norm_shift_in, out, totals_out,
     mix, gain, norm_gain, norm_shift, wg, cur, acc, psend, precv, pown, xsend, xrecv, hbuf, sc, held, tsend, trecv, esend, erecv,
     loc_sem, stream_send, z_recv, y_recv, gift_recv,
     p_send_s, p_recv_s, x_send_s, x_recv_s, halo_s,
     c_send_s, c_recv_s, t_send_s, t_recv_s, e_send_s, e_recv_s, out_sem) = refs
    tokens, chans = stream.shape
    half = tokens // 2
    halo = layers * REACH
    ahead = halo - REACH
    reach_rows = half + halo
    part_rows = half + ahead
    d_model = chans * tp_n
    alpha = (2.0 * layers) ** 0.25
    nx = tp_n // 2
    y, z, t = lax.axis_index("grp"), lax.axis_index("sp"), lax.axis_index("tp")
    core, x = lax.rem(t, 2), t // 2
    sib = t + 1 - 2 * core
    orders = arrival_orders(n)
    mine, other = core * half, (1 - core) * half
    mine = pl.multiple_of(mine, REACH)
    other = pl.multiple_of(other, REACH)

    def order(s):
        if not streamed:
            return jnp.int32(s)
        b = jnp.int32(0)
        for k in range(n):
            b = jnp.where(z == k, orders[k][s], b)
        return b

    def remote(src, dst, ssem, rsem, device):
        return pltpu.make_async_remote_copy(
            src_ref=src, dst_ref=dst, send_sem=ssem, recv_sem=rsem,
            device_id=device, device_id_type=MESH)

    barrier = pltpu.get_barrier_semaphore()

    def greet(device):
        pl.semaphore_signal(barrier, inc=1, device_id=device, device_id_type=MESH)

    for k in range(1, tp_n):
        greet((y, z, lax.rem(t + k, tp_n)))
    count = jnp.int32(tp_n - 1)
    if streamed:
        greet((1 - y, z, t))
        count = count + 1

    @pl.when(z > 0)
    def _():
        greet((y, z - 1, t))

    @pl.when(z < n - 1)
    def _():
        greet((y, z + 1, t))

    count = count + jnp.where(z > 0, 1, 0) + jnp.where(z < n - 1, 1, 0)
    rows = w_in.shape[1]
    copies = [pltpu.make_async_copy(stream, cur.at[pl.ds(halo, tokens)], loc_sem.at[0])]
    for m in range(2 * layers):
        src = (w_in, w_out)[m % 2].at[m // 2]
        if streamed:
            dst = wg.at[m, pl.ds(pl.multiple_of(z * rows, rows), rows)]
        else:
            dst = wg.at[m]
        copies.append(pltpu.make_async_copy(src, dst, loc_sem.at[1 + m]))
    for at, pair in enumerate(((mix_in, mix), (gain_in, gain), (norm_gain_in, norm_gain), (norm_shift_in, norm_shift))):
        copies.append(pltpu.make_async_copy(*pair, loc_sem.at[1 + 2 * layers + at]))
    for copy in copies:
        copy.start()

    pl.semaphore_wait(barrier, count)

    part = rows // 2
    cut = part // PIECES

    def span(base, q):
        return pl.ds(pl.multiple_of(base + q * cut, cut), cut)

    edge = (z == 0) | (z == n - 1)

    side_cols = chans // 2
    col_cut = side_cols // PIECES

    def by_columns(m):
        return m == 2 * layers - 1

    def columns(side, q):
        return pl.ds(pl.multiple_of(side * side_cols + q * col_cut, 128), col_cut)

    def block_rows(b):
        return pl.ds(pl.multiple_of(b * width, width), width)

    def piece(cols, m, b, side, q):
        if cols:
            return wg.at[m, block_rows(b), columns(side, q)]
        return wg.at[m, span(b * rows + side * part, q)]

    def own_piece(m, side, q):
        w = (w_in, w_out)[m % 2].at[m // 2]
        return w.at[:, columns(side, q)] if by_columns(m) else w.at[span(side * part, q)]

    def half_block(m, b, side):
        if by_columns(m):
            return wg.at[m, block_rows(b), pl.ds(pl.multiple_of(side * side_cols, 128), side_cols)]
        return wg.at[m, pl.ds(pl.multiple_of(b * rows + side * part, part), part)]

    def place(b, zt):
        return b - jnp.where(b > zt, 1, 0)

    def own_copy(m, side, q):
        src, dst = own_piece(m, y, q), piece(by_columns(m), m, z, y, q)
        zt = z + 2 * side - 1
        return remote(src, dst, stream_send.at[0], z_recv.at[m, place(z, zt), q], (y, zt, t))

    def rest_copy(m, q):
        src, dst = own_piece(m, 1 - y, q), piece(by_columns(m), m, z, 1 - y, q)
        return remote(src, dst, stream_send.at[0], y_recv.at[m, z],
                      (y, jnp.where(z == 0, 1, n - 2), t))

    def own_start(m, k, side):
        if not 0 <= k + 2 * side - 1 < n:
            return

        @pl.when(z == k)
        def _():
            for q in range(PIECES):
                own_copy(m, side, q).start()
            if m == 0 and side:
                halo_copy().start()
            if k in (0, n - 1):
                for q in range(PIECES):
                    rest_copy(m, q).start()

    def arrived(cols, m, b, q):
        ref = piece(cols, m, b, y, q)
        remote(ref, ref, stream_send.at[0], z_recv.at[m, place(b, z), q], (y, z, t)).wait_recv()

    def onward(cols, m, b, q):
        zt = jnp.where(b < z, z + 1, z - 1)
        ref = piece(cols, m, b, y, q)
        return (zt >= 0) & (zt < n), remote(
            ref, ref, stream_send.at[0], z_recv.at[m, place(b, zt), q], (y, zt, t))

    def whole(b):
        return ((z == 1) & (b == 0)) | ((z == n - 2) & (b == n - 1))

    def across(cols, m, b, q):
        ref = piece(cols, m, b, y, q)
        return remote(ref, ref, stream_send.at[0], y_recv.at[m, b], (1 - y, z, t))

    def by_place(values):
        picked = jnp.int32(values[0])
        for k in range(1, n):
            if values[k] != values[0]:
                picked = jnp.where(z == k, values[k], picked)
        return picked

    edge_events, inner_events = stream_plan(n, layers)
    state = [0, 0]

    def take(e_event, i_event):
        places = [k for k in range(n) if (e_event if k in (0, n - 1) else i_event)]

        cols = by_columns((e_event or i_event)[0])

        def go():
            vals = [(e_event if k in (0, n - 1) else i_event) or e_event or i_event for k in range(n)]
            m = by_place([v[0] for v in vals])
            b = by_place([orders[k][v[1]] for k, v in enumerate(vals)])
            q = by_place([v[2] for v in vals])
            there, copy = onward(cols, m, b, q)
            arrived(cols, m, b, q)
            pl.when(there)(copy.start)
            given = edge & (m == 2 * layers - 1) & (b == n - 1 - z) & (q >= PIECES - GIFT)
            pl.when(jnp.logical_not(whole(b) | given))(across(cols, m, b, q).start)

        if len(places) == n:
            go()
        else:
            pl.when(edge if e_event else jnp.logical_not(edge))(go)
        for k in places:
            m, s, q = e_event if k in (0, n - 1) else i_event
            if q != PIECES - 1 or m + 1 >= 2 * layers:
                continue
            if k in (0, n - 1):
                if s == 1:
                    own_start(m + 1, k, 1 if k == 0 else 0)
            elif s == n - 1:
                own_start(m + 1, k, 0 if k < n / 2 else 1)
            elif s == 2:
                own_start(m + 1, k, 1 if k < n / 2 else 0)

    def tick(e_goal, i_goal):
        if not streamed:
            return
        while state[0] < e_goal or state[1] < i_goal:
            e_event = i_event = None
            if state[0] < e_goal:
                e_event = edge_events[state[0]]
                state[0] += 1
            if state[1] < i_goal:
                i_event = inner_events[state[1]]
                state[1] += 1
            if e_event and i_event and by_columns(e_event[0]) != by_columns(i_event[0]):
                take(e_event, None)
                take(None, i_event)
            else:
                take(e_event, i_event)

    def ready(m, s):
        if s == 0:
            copies[1 + m].wait()
        elif streamed:
            b = order(s)
            ref = half_block(m, b, 1 - y)
            remote(ref, ref, stream_send.at[0], y_recv.at[m, b], (y, z, t)).wait_recv()

    def weight(m, s):
        return wg[m, pl.ds(pl.multiple_of(order(s) * width, width), width), :]

    def p_copy(l, s):
        return remote(psend.at[l, s], precv.at[l, s], p_send_s.at[0], p_recv_s.at[l, s], (y, z, sib))

    def x_copies(l, s):
        return [remote(xsend.at[l, s], xrecv.at[k - 1, l, s], x_send_s.at[0],
                       x_recv_s.at[k - 1, l, s], (y, z, lax.rem(x + k, nx) * 2 + core))
                for k in range(1, nx)]

    def halo_copy():
        return remote(stream.at[pl.ds(tokens - halo, halo)], cur.at[pl.ds(0, halo)],
                      halo_s.at[0], halo_s.at[1], (y, jnp.minimum(z + 1, n - 1), t))

    def c_copy(l, s, side):
        ref = sc.at[l, s, side]
        return remote(ref, ref, c_send_s.at[0], c_recv_s.at[l, s], (y, z, sib))

    def t_copies(l, i):
        return [remote(tsend.at[l, i], trecv.at[k - 1, l, i], t_send_s.at[0],
                       t_recv_s.at[l, i], (y, z, lax.rem(t + k, tp_n)))
                for k in range(1, tp_n)]

    def e_copies(l):
        return [remote(esend.at[l], erecv.at[k - 1, l], e_send_s.at[0],
                       e_recv_s.at[l], (y, z, lax.rem(t + k, tp_n)))
                for k in range(1, tp_n)]

    def settle(ref, sem):
        pltpu.make_async_copy(ref, ref, sem).wait()

    def project(l, s):
        w = weight(2 * l, s)
        psend[l, s] = lax.dot_general(
            cur[pl.ds(other, reach_rows), :], w, NT, preferred_element_type=F32).astype(BF16)
        p_copy(l, s).start()
        pown[s] = lax.dot_general(cur[pl.ds(mine, reach_rows), :], w, NT, preferred_element_type=F32)

    def chip_sum(l, s):
        p_copy(l, s).wait_recv()
        total = pown[s] + precv[l, s].astype(F32)
        pown[s] = total
        xsend[l, s] = total.astype(BF16)
        for copy in x_copies(l, s):
            copy.start()

    def finish_hidden(l, s):
        total = pown[s]
        for k, copy in enumerate(x_copies(l, s)):
            copy.wait_recv()
            total = total + xrecv[k, l, s].astype(F32)
        hbuf[s] = total.astype(BF16).astype(F32)

        @pl.when((z == 0) & (core == 0))
        def _():
            hbuf[s, :halo, :] = jnp.zeros((halo, width), F32)

    def pool(l, s):
        b = order(s)
        ext = hbuf[s]
        run = ext + pltpu.roll(ext, 1, 0)
        for octave in range(1, groups):
            take = jnp.where(b >= octave, 1.0, 0.0).astype(F32)
            run = run + take * pltpu.roll(run, 2**octave, 0)
        reach = jnp.int32(2)
        for octave in range(1, groups):
            reach = jnp.where(b >= octave, 2 ** (octave + 1), reach)
        at = z * tokens + core * half - ahead + 1 + lax.broadcasted_iota(jnp.int32, (part_rows, width), 0)
        counts = jnp.clip(at, 1, reach).astype(F32)
        pooled = (run[REACH:, :] / counts - ext[REACH:, :]).astype(BF16)
        mixed = jnp.dot(pooled, mix[l, b], preferred_element_type=F32)
        sc[l, s, core] = (mixed * gain[l:l + 1, pl.ds(pl.multiple_of(b * width, width), width)]).astype(BF16)
        c_copy(l, s, core).start()

    def grow(l, s, add, rows_at, cur_at):
        if s == 0:
            acc[rows_at, :] = alpha * cur[cur_at, :].astype(F32) + add
        else:
            acc[rows_at, :] = acc[rows_at, :] + add

    def row_totals(v):
        lane = lax.broadcasted_iota(jnp.int32, (v.shape[0], 128), 1)
        row_sum = jnp.sum(v, axis=1, keepdims=True)
        row_squares = jnp.sum(v * v, axis=1, keepdims=True)
        return jnp.where(lane == 0, row_sum, jnp.where(lane == 1, row_squares, 0.0))

    def expand(l, s):
        c_copy(l, s, 1 - core).wait_recv()
        at_m = 2 * l + 1
        extra = l * REACH

        if extra < ahead:
            add = jnp.dot(sc[l, s, 0, extra:ahead, :], weight(at_m, s), preferred_element_type=F32)
            grow(l, s, add, slice(extra, ahead), slice(extra + REACH, halo))
            if s == groups - 1:
                esend[l, extra:, :] = row_totals(acc[extra:ahead, :])
                for copy in e_copies(l):
                    copy.start()

        def body(i, carry):
            add = jnp.dot(sc[l, s, i, ahead:, :], weight(at_m, s), preferred_element_type=F32)
            at = i * half
            if not isinstance(i, int):
                at = pl.multiple_of(at, REACH)
            grow(l, s, add, pl.ds(ahead + at, half), pl.ds(halo + at, half))
            return carry

        if s < groups - 1:
            lax.fori_loop(0, 2, body, 0)
            return
        if l == layers - 1:
            side = lax.rem(y, 2)
            early = (PIECES - GIFT) * col_cut
            widen(l, s, side, 0, side_cols)
            if streamed:
                ready_last(at_m, s)
                gift()
            widen(l, s, 1 - side, 0, early)
            if streamed:
                ready_given(s)
            widen(l, s, 1 - side, early, side_cols - early)
            return
        for i in range(2):
            body(i, 0)
            both = row_totals(acc[ahead + i * half:ahead + (i + 1) * half, :])
            tsend[l, i] = both.T[:8, :]
            for copy in t_copies(l, i):
                copy.start()

    def widen(l, s, side, start, size):
        final = start > 0
        at = pl.ds(pl.multiple_of(side * side_cols + start, 128), size)
        w = wg[2 * l + 1, block_rows(order(s)), at]
        for i in range(2):
            r = pl.ds(ahead + i * half, half)
            v = acc[r, at] + jnp.dot(sc[l, s, i, ahead:, :], w, preferred_element_type=F32)
            acc[r, at] = v
            strips = [v[:, k:k + 128] for k in range(0, size, 128)]
            sums = functools.reduce(jnp.add, strips)
            squares = functools.reduce(jnp.add, [u * u for u in strips])
            if size < side_cols:
                sums, squares = held[0, i] + sums, held[1, i] + squares
            if not final:
                held[0, i], held[1, i] = sums, squares
                continue
            row_sum = jnp.sum(sums, axis=1, keepdims=True)
            row_squares = jnp.sum(squares, axis=1, keepdims=True)
            lane = lax.broadcasted_iota(jnp.int32, (half, 128), 1)
            both = jnp.where(lane == 0, row_sum, jnp.where(lane == 1, row_squares, 0.0))
            tsend[l, i] = both.T[:8, :]
            for copy in t_copies(l, i):
                copy.start()
            out_copy(i).start()

    def out_copy(i):
        return pltpu.make_async_copy(
            acc.at[pl.ds(ahead + i * half, half)], out.at[pl.ds(i * half, half)], out_sem.at[i])

    def norm(l, i):
        extra = l * REACH

        def apply(at, mean, inv, size):
            v = (acc[at:at + size, :] - mean) * inv
            to = at - ahead + halo
            cur[to:to + size, :] = (v * norm_gain[l:l + 1, :] + norm_shift[l:l + 1, :]).astype(BF16)

        if extra < ahead and i == 0:
            stats = esend[l, extra:, :]
            settle(erecv.at[:, l], e_recv_s.at[l])
            for k in range(tp_n - 1):
                stats = stats + erecv[k, l, extra:, :]
            stats = stats / d_model
            mean = stats[:, 0:1]
            inv = lax.rsqrt(stats[:, 1:2] - mean * mean + EPSILON)
            apply(extra, mean, inv, ahead - extra)
        stats = tsend[l, i]
        settle(trecv.at[:, l, i], t_recv_s.at[l, i])
        for k in range(tp_n - 1):
            stats = stats + trecv[k, l, i]
        if l == layers - 1:
            totals_out[:, i * half:(i + 1) * half] = stats
            return
        apply(ahead + i * half, *mean_and_scale(stats / d_model), half)


    if streamed:
        for k in range(n):
            for side in (1, 0):
                own_start(0, k, side)
    else:
        pl.when(z < n - 1)(halo_copy().start)

    def before_first():
        @pl.when(z > 0)
        def _():
            halo_copy().wait_recv()

        @pl.when(z == 0)
        def _():
            cur[:halo, :] = jnp.zeros((halo, chans), BF16)

        copies[0].wait()
        for copy in copies[1 + 2 * layers:]:
            copy.wait()

    def given_part(b, side):
        at = side * side_cols + (PIECES - GIFT) * col_cut
        return wg.at[2 * layers - 1, block_rows(b), pl.ds(pl.multiple_of(at, 128), GIFT * col_cut)]

    def gift():
        zt = jnp.where(z == 1, 0, n - 1)

        @pl.when(jnp.logical_not(edge))
        def _():
            ref = given_part(order(n - 1), 1 - y)
            remote(ref, ref, stream_send.at[0], gift_recv.at[0], (y, zt, t)).start()

    def ready_last(m, s):
        b = order(s)

        @pl.when(edge)
        def _():
            ref = wg.at[m, block_rows(b), pl.ds(pl.multiple_of((1 - y) * side_cols, 128), (PIECES - GIFT) * col_cut)]
            remote(ref, ref, stream_send.at[0], y_recv.at[m, b], (y, z, t)).wait_recv()

        @pl.when(jnp.logical_not(edge))
        def _():
            ready(m, s)

    def ready_given(s):
        @pl.when(edge)
        def _():
            ref = given_part(order(s), 1 - y)
            remote(ref, ref, stream_send.at[0], gift_recv.at[0], (y, z, t)).wait_recv()

    def drain():
        if streamed:
            given = GIFT * cut // (2 * layers)

            @pl.when(edge)
            def _():
                settle(wg.at[:, pl.ds(0, (n + 1) * part - given)], stream_send.at[0])

            @pl.when(jnp.logical_not(edge))
            def _():
                settle(wg.at[:, pl.ds(0, (2 * n - 1) * part + given)], stream_send.at[0])
        settle(psend, p_send_s.at[0])
        if nx > 1:
            settle(xrecv, x_send_s.at[0])
        settle(sc.at[:, :, core], c_send_s.at[0])
        settle(trecv, t_send_s.at[0])
        settle(erecv.at[:, pl.ds(0, layers - 1)], e_send_s.at[0])
        pl.when(z < n - 1)(halo_copy().wait_send)

    phases = {"project": project, "chip_sum": chip_sum, "finish_hidden": finish_hidden,
              "pool": pool, "expand": expand, "norm": norm}
    at = 0
    for l in range(layers):
        for name, s in STEPS:
            if at < len(EDGE_TICKS):
                tick(EDGE_TICKS[at], INNER_TICKS[at])
            if at == 0:
                before_first()
            if name == "project":
                ready(2 * l, s)
            elif name == "expand" and (l, s) != (layers - 1, groups - 1):
                ready(2 * l + 1, s)
            if l == layers - 1 and (name, s) == ("norm", 0):
                drain()
            phases[name](l, s)
            at += 1

    for i in range(2):
        out_copy(i).wait()


def per_device(n, grp_n, tp_n, stream, in_weight, out_weight, group_mix, pool_gain, norm_gain, norm_shift):
    layers, groups, width = group_mix.shape[:3]
    tokens, chans = stream.shape
    pool = groups * width
    streamed = n == groups == 4 and grp_n == 2 and layers == 2
    if not streamed:
        in_weight = lax.all_gather(in_weight, "sp", axis=1, tiled=True)
        out_weight = lax.all_gather(out_weight, "sp", axis=1, tiled=True)
    nx = tp_n // 2
    half = tokens // 2
    halo = layers * REACH
    ahead = halo - REACH
    ms = 2 * layers
    dma = pltpu.SemaphoreType.DMA
    any_spec = pl.BlockSpec(memory_space=pl.ANY)
    vmem = pl.BlockSpec(memory_space=pltpu.VMEM)
    xs = max(nx - 1, 1)
    summed, totals = pl.pallas_call(
        functools.partial(kernel, (n, tp_n, layers, groups, width, streamed)),
        out_shape=(jax.ShapeDtypeStruct((tokens, chans), F32), jax.ShapeDtypeStruct((8, tokens), F32)),
        in_specs=[any_spec] * 7,
        out_specs=(any_spec, vmem),
        scratch_shapes=[
            pltpu.VMEM(group_mix.shape, BF16),
            pltpu.VMEM(pool_gain.shape, F32),
            pltpu.VMEM(norm_gain.shape, F32),
            pltpu.VMEM(norm_shift.shape, F32),
            pltpu.VMEM((ms, pool, chans), BF16),
            pltpu.VMEM((halo + tokens, chans), BF16),
            pltpu.VMEM((ahead + tokens, chans), F32),
            pltpu.VMEM((layers, groups, halo + half, width), BF16),
            pltpu.VMEM((layers, groups, halo + half, width), BF16),
            pltpu.VMEM((groups, halo + half, width), F32),
            pltpu.VMEM((layers, groups, halo + half, width), BF16),
            pltpu.VMEM((xs, layers, groups, halo + half, width), BF16),
            pltpu.VMEM((groups, halo + half, width), F32),
            pltpu.VMEM((layers, groups, 2, ahead + half, width), BF16),
            pltpu.VMEM((2, 2, half, 128), F32),
            pltpu.VMEM((layers, 2, 8, half), F32),
            pltpu.VMEM((tp_n - 1, layers, 2, 8, half), F32),
            pltpu.VMEM((layers, ahead, 128), F32),
            pltpu.VMEM((tp_n - 1, layers, ahead, 128), F32),
            dma((5 + ms,)),
            dma((1,)), dma((ms, groups - 1, PIECES)), dma((ms, groups)), dma((1,)),
            dma((1,)), dma((layers, groups)),
            dma((1,)), dma((xs, layers, groups)),
            dma((2,)),
            dma((1,)), dma((layers, groups)),
            dma((1,)), dma((layers, 2)),
            dma((1,)), dma((layers,)),
            dma((2,)),
        ],
        compiler_params=pltpu.CompilerParams(
            collective_id=0, has_side_effects=True, vmem_limit_bytes=56 * 1024 * 1024),
    )(stream, in_weight, out_weight, group_mix,
      pool_gain, norm_gain, norm_shift)
    steps = tokens // (256 if tokens % 256 == 0 else 128)
    return pl.pallas_call(
        functools.partial(finish, chans * tp_n, layers - 1),
        out_shape=jax.ShapeDtypeStruct((tokens, chans), BF16),
        in_specs=[any_spec] * 4,
        out_specs=any_spec,
        scratch_shapes=[
            pltpu.VMEM((tokens, chans), F32),
            pltpu.VMEM((tokens, chans), BF16),
            pltpu.VMEM((8, tokens), F32),
            pltpu.VMEM(norm_gain.shape, F32),
            pltpu.VMEM(norm_shift.shape, F32),
            dma((steps,)),
            dma((steps,)),
            dma((3,)),
        ],
    )(summed, totals, norm_gain, norm_shift)


def solution(mesh):
    in_specs = (
        P(("grp", "sp"), "tp"),
        P(None, "sp", "tp"),
        P(None, "sp", "tp"),
        P(),
        P(),
        P(None, "tp"),
        P(None, "tp"),
    )
    out_specs = P(("grp", "sp"), "tp")
    sizes = mesh.shape
    body = functools.partial(per_device, sizes["sp"], sizes["grp"], sizes["tp"])
    return jax.shard_map(
        body, mesh=mesh, in_specs=in_specs, out_specs=out_specs, check_vma=False
    )
```

```python
import functools

import jax
import jax.numpy as jnp
from jax import lax
from jax.experimental import pallas as pl
from jax.experimental.pallas import tpu as pltpu
from jax.sharding import PartitionSpec as P

MESH = pl.DeviceIdType.MESH
EPSILON = 1e-05
F32 = jnp.float32
BF16 = jnp.bfloat16
REACH = 16
PIECES = 4
GIFT = 2
STEPS = (
    ("project", 0), ("chip_sum", 0), ("project", 1), ("chip_sum", 1), ("project", 2), ("chip_sum",
    2), ("project", 3), ("chip_sum", 3), ("finish_hidden", 0), ("pool", 0), ("finish_hidden", 1),
    ("pool", 1), ("expand", 0), ("finish_hidden", 2), ("pool", 2), ("expand", 1), ("finish_hidden",
    3), ("pool", 3), ("expand", 2), ("expand", 3), ("norm", 0), ("norm", 1),
)
EDGE_TICKS = (4, 6, 7, 9, 11, 13, 15, 17, 17, 17, 17, 17, 18, 19, 19, 19, 22, 22, 23, 27, 29, 30, 30, 32, 32,
    33, 35, 37, 39, 41, 41, 41, 41, 41, 42, 43, 43, 44, 47, 47, 47, 48, 48, 48)
INNER_TICKS = (8, 10, 11, 12, 12, 16, 18, 20, 20, 20, 22, 22, 22, 25, 25, 26, 30, 30, 31, 33, 35, 35, 35, 37,
    37, 38, 38, 40, 40, 40, 41, 41, 45, 45, 46, 48, 48, 48, 48, 48, 48, 48, 48, 48)
INNER_ORDER = (1, 2, 1, 2, 1, 2, 1, 2, 3, 3, 3, 3, 1, 2, 1, 2, 1, 2, 1, 2, 3, 3, 3, 3, 1, 1, 1, 2, 1, 2, 2, 3,
    2, 3, 3, 3, 1, 1, 1, 1, 2, 2, 2, 3, 2, 3, 3, 3)
NT = (((1,), (1,)), ((), ()))


def arrival_orders(n):
    orders = []
    for z in range(n):
        first = 1 if z < n / 2 else -1
        order = [z]
        for d in range(1, n):
            order += [b for b in (z + first * d, z - first * d) if 0 <= b < n]
        orders.append(order)
    return orders


def stream_plan(n, layers):
    ms = 2 * layers
    edge = [(m, s, q) for m in range(ms) for s in range(1, n) for q in range(PIECES)]
    seen = [0] * n
    inner = []
    for s in INNER_ORDER:
        inner.append((seen[s] // PIECES, s, seen[s] % PIECES))
        seen[s] += 1
    return edge, inner


def mean_and_scale(stats):
    mean = stats[0:1, :]
    inv = lax.rsqrt(stats[1:2, :] - mean * mean + EPSILON)
    row = lax.broadcasted_iota(jnp.int32, (128, stats.shape[1]), 0)
    cols = jnp.where(row == 0, mean, jnp.where(row == 1, inv, 0.0)).T
    return cols[:, 0:1], cols[:, 1:2]


def finish(d_model, last, summed, totals_in, gain_in, shift_in, out,
           held, ready, totals, norm_gain, norm_shift, in_sem, out_sem, side_sem):
    tokens = held.shape[0]
    size = 256 if tokens % 256 == 0 else 128
    blocks = [pl.ds(i * size, size) for i in range(tokens // size)]
    loads = [pltpu.make_async_copy(summed.at[r], held.at[r], in_sem.at[i]) for i, r in enumerate(blocks)]
    stores = [pltpu.make_async_copy(ready.at[r], out.at[r], out_sem.at[i]) for i, r in enumerate(blocks)]
    sides = [pltpu.make_async_copy(a, b, side_sem.at[i]) for i, (a, b) in enumerate(
        ((totals_in, totals), (gain_in, norm_gain), (shift_in, norm_shift)))]
    for load in sides + loads:
        load.start()
    for side in sides:
        side.wait()
    for i, r in enumerate(blocks):
        mean, inv = mean_and_scale(totals[:, i * size:(i + 1) * size] / d_model)
        loads[i].wait()
        v = (held[r, :] - mean) * inv
        ready[r, :] = (v * norm_gain[last:last + 1, :] + norm_shift[last:last + 1, :]).astype(BF16)
        stores[i].start()
    for store in stores:
        store.wait()


def kernel(cfg, *refs):
    n, tp_n, layers, groups, width, streamed = cfg
    (stream, w_in, w_out, mix_in, gain_in, norm_gain_in, norm_shift_in, out, totals_out,
     mix, gain, norm_gain, norm_shift, wg, cur, acc, psend, precv, pown, xsend, xrecv, hbuf, sc, held, tsend, trecv, esend, erecv,
     loc_sem, stream_send, z_recv, y_recv, gift_recv,
     p_send_s, p_recv_s, x_send_s, x_recv_s, halo_s,
     c_send_s, c_recv_s, t_send_s, t_recv_s, e_send_s, e_recv_s, out_sem) = refs
    tokens, chans = stream.shape
    half = tokens // 2
    halo = layers * REACH
    ahead = halo - REACH
    reach_rows = half + halo
    part_rows = half + ahead
    d_model = chans * tp_n
    alpha = (2.0 * layers) ** 0.25
    nx = tp_n // 2
    y, z, t = lax.axis_index("grp"), lax.axis_index("sp"), lax.axis_index("tp")
    core, x = lax.rem(t, 2), t // 2
    sib = t + 1 - 2 * core
    orders = arrival_orders(n)
    mine, other = core * half, (1 - core) * half
    mine = pl.multiple_of(mine, REACH)
    other = pl.multiple_of(other, REACH)

    def order(s):
        if not streamed:
            return jnp.int32(s)
        b = jnp.int32(0)
        for k in range(n):
            b = jnp.where(z == k, orders[k][s], b)
        return b

    def remote(src, dst, ssem, rsem, device):
        return pltpu.make_async_remote_copy(
            src_ref=src, dst_ref=dst, send_sem=ssem, recv_sem=rsem,
            device_id=device, device_id_type=MESH)

    barrier = pltpu.get_barrier_semaphore()

    def greet(device):
        pl.semaphore_signal(barrier, inc=1, device_id=device, device_id_type=MESH)

    for k in range(1, tp_n):
        greet((y, z, lax.rem(t + k, tp_n)))
    count = jnp.int32(tp_n - 1)
    if streamed:
        greet((1 - y, z, t))
        count = count + 1

    @pl.when(z > 0)
    def _():
        greet((y, z - 1, t))

    @pl.when(z < n - 1)
    def _():
        greet((y, z + 1, t))

    count = count + jnp.where(z > 0, 1, 0) + jnp.where(z < n - 1, 1, 0)
    rows = w_in.shape[1]
    copies = [pltpu.make_async_copy(stream, cur.at[pl.ds(halo, tokens)], loc_sem.at[0])]
    for m in range(2 * layers):
        src = (w_in, w_out)[m % 2].at[m // 2]
        if streamed:
            dst = wg.at[m, pl.ds(pl.multiple_of(z * rows, rows), rows)]
        else:
            dst = wg.at[m]
        copies.append(pltpu.make_async_copy(src, dst, loc_sem.at[1 + m]))
    for at, pair in enumerate(((mix_in, mix), (gain_in, gain), (norm_gain_in, norm_gain), (norm_shift_in, norm_shift))):
        copies.append(pltpu.make_async_copy(*pair, loc_sem.at[1 + 2 * layers + at]))
    for copy in copies:
        copy.start()

    pl.semaphore_wait(barrier, count)

    part = rows // 2
    cut = part // PIECES

    def span(base, q):
        return pl.ds(pl.multiple_of(base + q * cut, cut), cut)

    edge = (z == 0) | (z == n - 1)

    side_cols = chans // 2
    col_cut = side_cols // PIECES

    def by_columns(m):
        return m == 2 * layers - 1

    def columns(side, q):
        return pl.ds(pl.multiple_of(side * side_cols + q * col_cut, 128), col_cut)

    def block_rows(b):
        return pl.ds(pl.multiple_of(b * width, width), width)

    def piece(cols, m, b, side, q):
        if cols:
            return wg.at[m, block_rows(b), columns(side, q)]
        return wg.at[m, span(b * rows + side * part, q)]

    def own_piece(m, side, q):
        w = (w_in, w_out)[m % 2].at[m // 2]
        return w.at[:, columns(side, q)] if by_columns(m) else w.at[span(side * part, q)]

    def half_block(m, b, side):
        if by_columns(m):
            return wg.at[m, block_rows(b), pl.ds(pl.multiple_of(side * side_cols, 128), side_cols)]
        return wg.at[m, pl.ds(pl.multiple_of(b * rows + side * part, part), part)]

    def place(b, zt):
        return b - jnp.where(b > zt, 1, 0)

    def own_copy(m, side, q):
        src, dst = own_piece(m, y, q), piece(by_columns(m), m, z, y, q)
        zt = z + 2 * side - 1
        return remote(src, dst, stream_send.at[0], z_recv.at[m, place(z, zt), q], (y, zt, t))

    def rest_copy(m, q):
        src, dst = own_piece(m, 1 - y, q), piece(by_columns(m), m, z, 1 - y, q)
        return remote(src, dst, stream_send.at[0], y_recv.at[m, place(z, jnp.where(z == 0, 1, n - 2))],
                      (y, jnp.where(z == 0, 1, n - 2), t))

    def own_start(m, k, side):
        if not 0 <= k + 2 * side - 1 < n:
            return

        @pl.when(z == k)
        def _():
            for q in range(PIECES):
                own_copy(m, side, q).start()
            if m == 0 and side:
                halo_copy().start()
            if k in (0, n - 1):
                for q in range(PIECES):
                    rest_copy(m, q).start()

    def arrived(cols, m, b, q):
        ref = piece(cols, m, b, y, q)
        remote(ref, ref, stream_send.at[0], z_recv.at[m, place(b, z), q], (y, z, t)).wait_recv()

    def onward(cols, m, b, q):
        zt = jnp.where(b < z, z + 1, z - 1)
        ref = piece(cols, m, b, y, q)
        return (zt >= 0) & (zt < n), remote(
            ref, ref, stream_send.at[0], z_recv.at[m, place(b, zt), q], (y, zt, t))

    def whole(b):
        return ((z == 1) & (b == 0)) | ((z == n - 2) & (b == n - 1))

    def across(cols, m, b, q):
        ref = piece(cols, m, b, y, q)
        return remote(ref, ref, stream_send.at[0], y_recv.at[m, place(b, z)], (1 - y, z, t))

    def by_place(values):
        picked = jnp.int32(values[0])
        for k in range(1, n):
            if values[k] != values[0]:
                picked = jnp.where(z == k, values[k], picked)
        return picked

    edge_events, inner_events = stream_plan(n, layers)
    state = [0, 0]

    def take(e_event, i_event):
        places = [k for k in range(n) if (e_event if k in (0, n - 1) else i_event)]

        cols = by_columns((e_event or i_event)[0])

        def go():
            vals = [(e_event if k in (0, n - 1) else i_event) or e_event or i_event for k in range(n)]
            m = by_place([v[0] for v in vals])
            b = by_place([orders[k][v[1]] for k, v in enumerate(vals)])
            q = by_place([v[2] for v in vals])
            there, copy = onward(cols, m, b, q)
            arrived(cols, m, b, q)
            pl.when(there)(copy.start)
            given = edge & (m == 2 * layers - 1) & (b == n - 1 - z) & (q >= PIECES - GIFT)
            pl.when(jnp.logical_not(whole(b) | given))(across(cols, m, b, q).start)

        if len(places) == n:
            go()
        else:
            pl.when(edge if e_event else jnp.logical_not(edge))(go)
        for k in places:
            m, s, q = e_event if k in (0, n - 1) else i_event
            if q != PIECES - 1 or m + 1 >= 2 * layers:
                continue
            if k in (0, n - 1):
                if s == 1:
                    own_start(m + 1, k, 1 if k == 0 else 0)
            elif s == n - 1:
                own_start(m + 1, k, 0 if k < n / 2 else 1)
            elif s == 2:
                own_start(m + 1, k, 1 if k < n / 2 else 0)

    def tick(e_goal, i_goal):
        if not streamed:
            return
        while state[0] < e_goal or state[1] < i_goal:
            e_event = i_event = None
            if state[0] < e_goal:
                e_event = edge_events[state[0]]
                state[0] += 1
            if state[1] < i_goal:
                i_event = inner_events[state[1]]
                state[1] += 1
            if e_event and i_event and by_columns(e_event[0]) != by_columns(i_event[0]):
                take(e_event, None)
                take(None, i_event)
            else:
                take(e_event, i_event)

    def ready(m, s):
        if s == 0:
            copies[1 + m].wait()
        elif streamed:
            b = order(s)
            ref = half_block(m, b, 1 - y)
            remote(ref, ref, stream_send.at[0], y_recv.at[m, place(b, z)], (y, z, t)).wait_recv()

    def weight(m, s):
        return wg[m, pl.ds(pl.multiple_of(order(s) * width, width), width), :]

    def p_copy(l, s):
        return remote(psend.at[l, s], precv.at[l, s], p_send_s.at[0], p_recv_s.at[s], (y, z, sib))

    def x_copies(l, s):
        return [remote(xsend.at[l, s], xrecv.at[k - 1, l, s], x_send_s.at[0],
                       x_recv_s.at[k - 1, s], (y, z, lax.rem(x + k, nx) * 2 + core))
                for k in range(1, nx)]

    def halo_copy():
        return remote(stream.at[pl.ds(tokens - halo, halo)], cur.at[pl.ds(0, halo)],
                      halo_s.at[0], halo_s.at[1], (y, jnp.minimum(z + 1, n - 1), t))

    def c_copy(l, s, side):
        ref = sc.at[l, s, side]
        return remote(ref, ref, c_send_s.at[0], c_recv_s.at[s], (y, z, sib))

    def t_copies(l, i):
        return [remote(tsend.at[l, i], trecv.at[k - 1, l, i], t_send_s.at[0],
                       t_recv_s.at[l, i], (y, z, lax.rem(t + k, tp_n)))
                for k in range(1, tp_n)]

    def e_copies(l):
        return [remote(esend.at[l], erecv.at[k - 1, l], e_send_s.at[0],
                       e_recv_s.at[l], (y, z, lax.rem(t + k, tp_n)))
                for k in range(1, tp_n)]

    def settle(ref, sem):
        pltpu.make_async_copy(ref, ref, sem).wait()

    def project(l, s):
        w = weight(2 * l, s)
        psend[l, s] = lax.dot_general(
            cur[pl.ds(other, reach_rows), :], w, NT, preferred_element_type=F32).astype(BF16)
        p_copy(l, s).start()
        pown[s] = lax.dot_general(cur[pl.ds(mine, reach_rows), :], w, NT, preferred_element_type=F32)

    def chip_sum(l, s):
        p_copy(l, s).wait_recv()
        total = pown[s] + precv[l, s].astype(F32)
        pown[s] = total
        xsend[l, s] = total.astype(BF16)
        for copy in x_copies(l, s):
            copy.start()

    def finish_hidden(l, s):
        total = pown[s]
        for k, copy in enumerate(x_copies(l, s)):
            copy.wait_recv()
            total = total + xrecv[k, l, s].astype(F32)
        hbuf[s] = total.astype(BF16).astype(F32)

        @pl.when((z == 0) & (core == 0))
        def _():
            hbuf[s, :halo, :] = jnp.zeros((halo, width), F32)

    def pool(l, s):
        b = order(s)
        ext = hbuf[s]
        run = ext + pltpu.roll(ext, 1, 0)
        for octave in range(1, groups):
            take = jnp.where(b >= octave, 1.0, 0.0).astype(F32)
            run = run + take * pltpu.roll(run, 2**octave, 0)
        reach = jnp.int32(2)
        for octave in range(1, groups):
            reach = jnp.where(b >= octave, 2 ** (octave + 1), reach)
        at = z * tokens + core * half - ahead + 1 + lax.broadcasted_iota(jnp.int32, (part_rows, width), 0)
        counts = jnp.clip(at, 1, reach).astype(F32)
        pooled = (run[REACH:, :] / counts - ext[REACH:, :]).astype(BF16)
        mixed = jnp.dot(pooled, mix[l, b], preferred_element_type=F32)
        sc[l, s, core] = (mixed * gain[l:l + 1, pl.ds(pl.multiple_of(b * width, width), width)]).astype(BF16)
        c_copy(l, s, core).start()

    def grow(l, s, add, rows_at, cur_at):
        if s == 0:
            acc[rows_at, :] = alpha * cur[cur_at, :].astype(F32) + add
        else:
            acc[rows_at, :] = acc[rows_at, :] + add

    def row_totals(v):
        lane = lax.broadcasted_iota(jnp.int32, (v.shape[0], 128), 1)
        row_sum = jnp.sum(v, axis=1, keepdims=True)
        row_squares = jnp.sum(v * v, axis=1, keepdims=True)
        return jnp.where(lane == 0, row_sum, jnp.where(lane == 1, row_squares, 0.0))

    def expand(l, s):
        c_copy(l, s, 1 - core).wait_recv()
        at_m = 2 * l + 1
        extra = l * REACH

        if extra < ahead:
            add = jnp.dot(sc[l, s, 0, extra:ahead, :], weight(at_m, s), preferred_element_type=F32)
            grow(l, s, add, slice(extra, ahead), slice(extra + REACH, halo))
            if s == groups - 1:
                esend[l, extra:, :] = row_totals(acc[extra:ahead, :])
                for copy in e_copies(l):
                    copy.start()

        def body(i, carry):
            add = jnp.dot(sc[l, s, i, ahead:, :], weight(at_m, s), preferred_element_type=F32)
            at = i * half
            if not isinstance(i, int):
                at = pl.multiple_of(at, REACH)
            grow(l, s, add, pl.ds(ahead + at, half), pl.ds(halo + at, half))
            return carry

        if s < groups - 1:
            lax.fori_loop(0, 2, body, 0)
            return
        if l == layers - 1:
            side = lax.rem(y, 2)
            early = (PIECES - GIFT) * col_cut
            widen(l, s, side, 0, side_cols)
            if streamed:
                ready_last(at_m, s)
                gift()
            widen(l, s, 1 - side, 0, early)
            if streamed:
                ready_given(s)
            widen(l, s, 1 - side, early, side_cols - early)
            return
        for i in range(2):
            body(i, 0)
            both = row_totals(acc[ahead + i * half:ahead + (i + 1) * half, :])
            tsend[l, i] = both.T[:8, :]
            for copy in t_copies(l, i):
                copy.start()

    def widen(l, s, side, start, size):
        final = start > 0
        at = pl.ds(pl.multiple_of(side * side_cols + start, 128), size)
        w = wg[2 * l + 1, block_rows(order(s)), at]
        for i in range(2):
            r = pl.ds(ahead + i * half, half)
            v = acc[r, at] + jnp.dot(sc[l, s, i, ahead:, :], w, preferred_element_type=F32)
            acc[r, at] = v
            strips = [v[:, k:k + 128] for k in range(0, size, 128)]
            sums = functools.reduce(jnp.add, strips)
            squares = functools.reduce(jnp.add, [u * u for u in strips])
            if size < side_cols:
                sums, squares = held[0, i] + sums, held[1, i] + squares
            if not final:
                held[0, i], held[1, i] = sums, squares
                continue
            row_sum = jnp.sum(sums, axis=1, keepdims=True)
            row_squares = jnp.sum(squares, axis=1, keepdims=True)
            lane = lax.broadcasted_iota(jnp.int32, (half, 128), 1)
            both = jnp.where(lane == 0, row_sum, jnp.where(lane == 1, row_squares, 0.0))
            tsend[l, i] = both.T[:8, :]
            for copy in t_copies(l, i):
                copy.start()
            out_copy(i).start()

    def out_copy(i):
        return pltpu.make_async_copy(
            acc.at[pl.ds(ahead + i * half, half)], out.at[pl.ds(i * half, half)], out_sem.at[i])

    def norm(l, i):
        extra = l * REACH

        def apply(at, mean, inv, size):
            v = (acc[at:at + size, :] - mean) * inv
            to = at - ahead + halo
            cur[to:to + size, :] = (v * norm_gain[l:l + 1, :] + norm_shift[l:l + 1, :]).astype(BF16)

        if extra < ahead and i == 0:
            stats = esend[l, extra:, :]
            settle(erecv.at[:, l], e_recv_s.at[l])
            for k in range(tp_n - 1):
                stats = stats + erecv[k, l, extra:, :]
            stats = stats / d_model
            mean = stats[:, 0:1]
            inv = lax.rsqrt(stats[:, 1:2] - mean * mean + EPSILON)
            apply(extra, mean, inv, ahead - extra)
        stats = tsend[l, i]
        settle(trecv.at[:, l, i], t_recv_s.at[l, i])
        for k in range(tp_n - 1):
            stats = stats + trecv[k, l, i]
        if l == layers - 1:
            totals_out[:, i * half:(i + 1) * half] = stats
            return
        apply(ahead + i * half, *mean_and_scale(stats / d_model), half)


    if streamed:
        for k in range(n):
            for side in (1, 0):
                own_start(0, k, side)
    else:
        pl.when(z < n - 1)(halo_copy().start)

    def before_first():
        @pl.when(z > 0)
        def _():
            halo_copy().wait_recv()

        @pl.when(z == 0)
        def _():
            cur[:halo, :] = jnp.zeros((halo, chans), BF16)

        copies[0].wait()
        for copy in copies[1 + 2 * layers:]:
            copy.wait()

    def given_part(b, side):
        at = side * side_cols + (PIECES - GIFT) * col_cut
        return wg.at[2 * layers - 1, block_rows(b), pl.ds(pl.multiple_of(at, 128), GIFT * col_cut)]

    def gift():
        zt = jnp.where(z == 1, 0, n - 1)

        @pl.when(jnp.logical_not(edge))
        def _():
            ref = given_part(order(n - 1), 1 - y)
            remote(ref, ref, stream_send.at[0], gift_recv.at[0], (y, zt, t)).start()

    def ready_last(m, s):
        b = order(s)

        @pl.when(edge)
        def _():
            ref = wg.at[m, block_rows(b), pl.ds(pl.multiple_of((1 - y) * side_cols, 128), (PIECES - GIFT) * col_cut)]
            remote(ref, ref, stream_send.at[0], y_recv.at[m, place(b, z)], (y, z, t)).wait_recv()

        @pl.when(jnp.logical_not(edge))
        def _():
            ready(m, s)

    def ready_given(s):
        @pl.when(edge)
        def _():
            ref = given_part(order(s), 1 - y)
            remote(ref, ref, stream_send.at[0], gift_recv.at[0], (y, z, t)).wait_recv()

    def drain():
        if streamed:
            given = GIFT * cut // (2 * layers)

            @pl.when(edge)
            def _():
                settle(wg.at[:, pl.ds(0, (n + 1) * part - given)], stream_send.at[0])

            @pl.when(jnp.logical_not(edge))
            def _():
                settle(wg.at[:, pl.ds(0, (2 * n - 1) * part + given)], stream_send.at[0])
        settle(psend, p_send_s.at[0])
        if nx > 1:
            settle(xrecv, x_send_s.at[0])
        settle(sc.at[:, :, core], c_send_s.at[0])
        settle(trecv, t_send_s.at[0])
        settle(erecv.at[:, pl.ds(0, layers - 1)], e_send_s.at[0])
        pl.when(z < n - 1)(halo_copy().wait_send)

    phases = {"project": project, "chip_sum": chip_sum, "finish_hidden": finish_hidden,
              "pool": pool, "expand": expand, "norm": norm}
    at = 0
    for l in range(layers):
        for name, s in STEPS:
            if at < len(EDGE_TICKS):
                tick(EDGE_TICKS[at], INNER_TICKS[at])
            if at == 0:
                before_first()
            if name == "project":
                ready(2 * l, s)
            elif name == "expand" and (l, s) != (layers - 1, groups - 1):
                ready(2 * l + 1, s)
            if l == layers - 1 and (name, s) == ("norm", 0):
                drain()
            phases[name](l, s)
            at += 1

    for i in range(2):
        out_copy(i).wait()


def per_device(n, grp_n, tp_n, stream, in_weight, out_weight, group_mix, pool_gain, norm_gain, norm_shift):
    layers, groups, width = group_mix.shape[:3]
    tokens, chans = stream.shape
    pool = groups * width
    streamed = n == groups == 4 and grp_n == 2 and layers == 2
    if not streamed:
        in_weight = lax.all_gather(in_weight, "sp", axis=1, tiled=True)
        out_weight = lax.all_gather(out_weight, "sp", axis=1, tiled=True)
    nx = tp_n // 2
    half = tokens // 2
    halo = layers * REACH
    ahead = halo - REACH
    ms = 2 * layers
    dma = pltpu.SemaphoreType.DMA
    any_spec = pl.BlockSpec(memory_space=pl.ANY)
    vmem = pl.BlockSpec(memory_space=pltpu.VMEM)
    xs = max(nx - 1, 1)
    summed, totals = pl.pallas_call(
        functools.partial(kernel, (n, tp_n, layers, groups, width, streamed)),
        out_shape=(jax.ShapeDtypeStruct((tokens, chans), F32), jax.ShapeDtypeStruct((8, tokens), F32)),
        in_specs=[any_spec] * 7,
        out_specs=(any_spec, vmem),
        scratch_shapes=[
            pltpu.VMEM(group_mix.shape, BF16),
            pltpu.VMEM(pool_gain.shape, F32),
            pltpu.VMEM(norm_gain.shape, F32),
            pltpu.VMEM(norm_shift.shape, F32),
            pltpu.VMEM((ms, pool, chans), BF16),
            pltpu.VMEM((halo + tokens, chans), BF16),
            pltpu.VMEM((ahead + tokens, chans), F32),
            pltpu.VMEM((layers, groups, halo + half, width), BF16),
            pltpu.VMEM((layers, groups, halo + half, width), BF16),
            pltpu.VMEM((groups, halo + half, width), F32),
            pltpu.VMEM((layers, groups, halo + half, width), BF16),
            pltpu.VMEM((xs, layers, groups, halo + half, width), BF16),
            pltpu.VMEM((groups, halo + half, width), F32),
            pltpu.VMEM((layers, groups, 2, ahead + half, width), BF16),
            pltpu.VMEM((2, 2, half, 128), F32),
            pltpu.VMEM((layers, 2, 8, half), F32),
            pltpu.VMEM((tp_n - 1, layers, 2, 8, half), F32),
            pltpu.VMEM((layers, ahead, 128), F32),
            pltpu.VMEM((tp_n - 1, layers, ahead, 128), F32),
            dma((5 + ms,)),
            dma((1,)), dma((ms, groups - 1, PIECES)), dma((ms, groups - 1)), dma((1,)),
            dma((1,)), dma((groups,)),
            dma((1,)), dma((xs, groups)),
            dma((2,)),
            dma((1,)), dma((groups,)),
            dma((1,)), dma((layers, 2)),
            dma((1,)), dma((layers,)),
            dma((2,)),
        ],
        compiler_params=pltpu.CompilerParams(
            collective_id=0, has_side_effects=True, vmem_limit_bytes=56 * 1024 * 1024),
    )(stream, in_weight, out_weight, group_mix,
      pool_gain, norm_gain, norm_shift)
    steps = tokens // (256 if tokens % 256 == 0 else 128)
    return pl.pallas_call(
        functools.partial(finish, chans * tp_n, layers - 1),
        out_shape=jax.ShapeDtypeStruct((tokens, chans), BF16),
        in_specs=[any_spec] * 4,
        out_specs=any_spec,
        scratch_shapes=[
            pltpu.VMEM((tokens, chans), F32),
            pltpu.VMEM((tokens, chans), BF16),
            pltpu.VMEM((8, tokens), F32),
            pltpu.VMEM(norm_gain.shape, F32),
            pltpu.VMEM(norm_shift.shape, F32),
            dma((steps,)),
            dma((steps,)),
            dma((3,)),
        ],
    )(summed, totals, norm_gain, norm_shift)


def solution(mesh):
    in_specs = (
        P(("grp", "sp"), "tp"),
        P(None, "sp", "tp"),
        P(None, "sp", "tp"),
        P(),
        P(),
        P(None, "tp"),
        P(None, "tp"),
    )
    out_specs = P(("grp", "sp"), "tp")
    sizes = mesh.shape
    body = functools.partial(per_device, sizes["sp"], sizes["grp"], sizes["tp"])
    return jax.shard_map(
        body, mesh=mesh, in_specs=in_specs, out_specs=out_specs, check_vma=False
    )
```
